32 devices in a mesh: kv: 8 (over z, y), tp: 4 (over x, core).
Axes of the slice: x: 2, y: 2, z: 4, core: 2. Of those that a mesh axis runs over, the one named last changes fastest.
Arguments:
- tokens: bfloat16 [160, 4096], P(None, 'kv'), may hold values from -40 to 40
- input_norm_gain: float32 [4096], P('kv'), may hold values from 0.1 to 1.9
- input_matrix: bfloat16 [4096, 4096], P('kv', 'tp'), may hold values from -0.09375 to 0.09375
- gate_matrix: bfloat16 [4096, 4096], P('kv', 'tp'), may hold values from -0.09375 to 0.09375
- write_matrix: bfloat16 [4096, 1024], P('kv', 'tp'), may hold values from -0.09375 to 0.09375
- read_matrix: bfloat16 [4096, 1024], P('kv', 'tp'), may hold values from -0.09375 to 0.09375
- step_matrix: bfloat16 [4096, 64], replicated, may hold values from -0.09375 to 0.09375
- input_kernel: float32 [4, 4096], P(None, 'tp'), may hold values from -3 to 3
- write_kernel: float32 [4, 1024], P(None, 'tp'), may hold values from -3 to 3
- read_kernel: float32 [4, 1024], P(None, 'tp'), may hold values from -3 to 3
- step_size_bias: float32 [64], P('tp'), may hold values from -6 to 1
- head_decay_logs: float32 [64], P('tp'), may hold values from 0 to 2.77
- bypass_scale: float32 [64], P('tp'), may hold values from 0.5 to 1.5
- extra_decay_logs: float32 [160, 64], P('kv', 'tp'), may hold values from -0.7 to 0, as said below
- output_norm_gain: float32 [4096], P('tp'), may hold values from 0.1 to 1.9
- output_matrix: bfloat16 [4096, 4096], P('tp', 'kv'), may hold values from -0.09375 to 0.09375
- cached_state_history: float32 [32, 6, 64, 64, 128], P('kv', None, 'tp'), may hold values from -2 to 2
- cached_input_rows: bfloat16 [32, 8, 4096], P('kv', None, 'tp'), may hold values from -6 to 6
- cached_write_rows: bfloat16 [32, 8, 1024], P('kv', None, 'tp'), may hold values from -6 to 6
- cached_read_rows: bfloat16 [32, 8, 1024], P('kv', None, 'tp'), may hold values from -6 to 6
- accepted: int32 [32], P('kv'), may hold values from 0 to 5
Outputs:
- mixer_out: bfloat16 [160, 4096], P('tp', 'kv')
- next_states: float32 [32, 6, 64, 64, 128], P('kv', None, 'tp')
- next_input: bfloat16 [32, 8, 4096], P('kv', None, 'tp')
- next_write: bfloat16 [32, 8, 1024], P('kv', None, 'tp')
- next_read: bfloat16 [32, 8, 1024], P('kv', None, 'tp')
The draws below stay inside these ranges and needn't reach their ends.
Inputs may be any that keep to these rules, and one draw needn't show every extreme that they name: `extra_decay_logs`: zero at most tokens and heads.
All inputs are finite; a program needn't handle non-finite values.
Results may differ from the reference program's by a relative error of at most 0.03.
Values may be sent and summed in bfloat16 or wider, within the bound.
A program may use at most 64 MiB of HBM per device.

```python
import math
import jax
import jax.numpy as jnp
from jax import lax

D = 4096
HEAD_TOTAL = 64
P_SIZE = 64
N = 128
G = 8
TAPS = 4
DRAFT_TOKENS = 5
SEQUENCE_TOTAL = 32
TOKENS = 160
N_TP = 4


def draw_tokens(key, part):
    first, second, third = jax.random.split(jax.random.fold_in(key, 11), 3)
    column = jnp.arange(D, dtype=jnp.float32)
    column_scale = jnp.exp(math.log(3.0) * column / max(D - 1, 1)) * jnp.exp(jax.random.uniform(second, (D,), jnp.float32, -0.35, 0.35))
    base = jax.random.normal(first, (TOKENS, D), jnp.float32)
    row_scale = jnp.exp(jax.random.uniform(third, (TOKENS, 1), jnp.float32, math.log(0.3), math.log(3.0)))
    values = jnp.clip(base * row_scale * column_scale[None, :], -40.0, 40.0)
    return values.astype(jnp.bfloat16)


def draw_extra_decay_logs(key, part):
    first, second = jax.random.split(jax.random.fold_in(key, 23), 2)
    struck = jax.random.randint(first, (TOKENS, HEAD_TOTAL), 0, 4) == 0
    depth = jax.random.uniform(second, (TOKENS, HEAD_TOTAL), jnp.float32, -0.5, -0.22)
    return jnp.where(struck, depth, 0.0).astype(jnp.float32)


def touch_ends(result, key, low, high):
    longest = result.shape.index(max(result.shape))
    spots = []
    for shift in (0, 1):
        where = [jax.random.randint(jax.random.fold_in(key, axis), (), 0, length) for axis, length in enumerate(result.shape)]
        where[longest] = (where[longest] + shift) % result.shape[longest]
        spots.append(tuple(where))
    return result.at[spots[0]].set(low).at[spots[1]].set(high)


def block_levels(rng, dims, cuts, low, top_value):
    gain = 1.0
    for dim, parts in cuts:
        draws = jax.random.uniform(jax.random.fold_in(jax.random.fold_in(rng, 6), dim), (parts,), jnp.float32, low / len(cuts), top_value / len(cuts))
        gain = gain * jnp.repeat(jnp.exp(draws), dims[dim] // parts).reshape((-1,) + (1,) * (len(dims) - 1 - dim))
    return gain


def gaussian(own_key, extent, width, reach, cuts=(), kind=jnp.bfloat16):
    values = jax.random.normal(own_key, extent, jnp.float32) * width
    if len(cuts) > 0:
        values = block_levels(own_key, extent, cuts, -0.22, 0.18) * values
    return jnp.clip(values, min=-reach, max=reach).astype(kind)


def setup_inputs(seed: int = 0) -> dict:
    key_list = jax.random.split(jax.random.key(seed), 22)
    return {
        "tokens": draw_tokens(jax.random.fold_in(key_list[21], 71), 0),
        "input_norm_gain": jnp.clip(1.0 + 0.18 * jax.random.normal(key_list[1], (D,), jnp.float32), 0.1, 1.9),
        "input_matrix": gaussian(key_list[2], (D, HEAD_TOTAL * P_SIZE), D ** -0.5, 0.09375, ((0, 8), (1, 4))),
        "gate_matrix": gaussian(key_list[3], (D, HEAD_TOTAL * P_SIZE), D ** -0.5, 0.09375, ((0, 8), (1, 4))),
        "write_matrix": gaussian(key_list[4], (D, G * N), D ** -0.5, 0.09375, ((0, 8), (1, 4))),
        "read_matrix": gaussian(key_list[5], (D, G * N), D ** -0.5, 0.09375, ((0, 8), (1, 4))),
        "step_matrix": gaussian(key_list[6], (D, HEAD_TOTAL), D ** -0.5, 0.09375),
        "input_kernel": gaussian(key_list[7], (TAPS, HEAD_TOTAL * P_SIZE), 0.5, 3.0, ((1, 4),), jnp.float32),
        "write_kernel": gaussian(key_list[8], (TAPS, G * N), 0.5, 3.0, ((1, 4),), jnp.float32),
        "read_kernel": gaussian(key_list[9], (TAPS, G * N), 0.5, 3.0, ((1, 4),), jnp.float32),
        "step_size_bias": jnp.clip(-6.0 + 7.0 * jax.random.uniform(key_list[10], (HEAD_TOTAL,), jnp.float32) ** block_levels(key_list[10], (HEAD_TOTAL,), ((0, 4),), -0.2, 0.2), -6.0, 1.0),
        "head_decay_logs": jnp.clip(2.77 * jax.random.uniform(key_list[11], (HEAD_TOTAL,), jnp.float32) ** block_levels(key_list[11], (HEAD_TOTAL,), ((0, 4),), -0.2, 0.2), 0.0, 2.77),
        "bypass_scale": jnp.clip(0.5 + 1.0 * jax.random.uniform(key_list[12], (HEAD_TOTAL,), jnp.float32) ** block_levels(key_list[12], (HEAD_TOTAL,), ((0, 4),), -0.2, 0.2), 0.5, 1.5),
        "extra_decay_logs": draw_extra_decay_logs(jax.random.fold_in(key_list[21], 71), 0),
        "output_norm_gain": jnp.clip(1.0 + 0.18 * jax.random.normal(key_list[14], (HEAD_TOTAL * P_SIZE,), jnp.float32), 0.1, 1.9),
        "output_matrix": gaussian(key_list[15], (HEAD_TOTAL * P_SIZE, D), (HEAD_TOTAL * P_SIZE) ** -0.5, 0.09375, ((0, 4), (1, 8))),
        "cached_state_history": gaussian(key_list[16], (SEQUENCE_TOTAL, DRAFT_TOKENS + 1, HEAD_TOTAL, P_SIZE, N), 0.3, 2.0, ((0, 8), (2, 4)), jnp.float32),
        "cached_input_rows": gaussian(key_list[17], (SEQUENCE_TOTAL, DRAFT_TOKENS + TAPS - 1, HEAD_TOTAL * P_SIZE), 1.0, 6.0, ((0, 8), (2, 4))),
        "cached_write_rows": gaussian(key_list[18], (SEQUENCE_TOTAL, DRAFT_TOKENS + TAPS - 1, G * N), 1.0, 6.0, ((0, 8), (2, 4))),
        "cached_read_rows": gaussian(key_list[19], (SEQUENCE_TOTAL, DRAFT_TOKENS + TAPS - 1, G * N), 1.0, 6.0, ((0, 8), (2, 4))),
        "accepted": touch_ends(jax.random.randint(key_list[20], (SEQUENCE_TOTAL,), 0, DRAFT_TOKENS + 1), jax.random.fold_in(key_list[20], 1), 0, DRAFT_TOKENS).astype(jnp.int32),
    }


epsilon = 1e-05

def make_window(saved, fresh, accepted):
    offsets = jnp.arange(TAPS - 1, dtype=jnp.int32)
    index = (accepted[:, None] + offsets[None, :]).astype(jnp.int32)
    taken_rows = jnp.take_along_axis(saved, index[:, :, None], axis=1)
    return jnp.concatenate([taken_rows, fresh.reshape(SEQUENCE_TOTAL, DRAFT_TOKENS, -1)], axis=1)

def convolve(window, taps):
    total = jnp.zeros((window.shape[0], DRAFT_TOKENS, window.shape[2]), jnp.float32)
    for tap_index in range(TAPS):
        total = total + taps[tap_index] * window[:, tap_index:tap_index + DRAFT_TOKENS].astype(jnp.float32)
    return jax.nn.silu(total)

def reference(tokens, input_norm_gain, input_matrix, gate_matrix, write_matrix, read_matrix, step_matrix, input_kernel, write_kernel, read_kernel, step_size_bias, head_decay_logs, bypass_scale, extra_decay_logs, output_norm_gain, output_matrix, cached_state_history, cached_input_rows, cached_write_rows, cached_read_rows, accepted):
    wide_rows = tokens.astype(jnp.float32)
    inverse = lax.rsqrt(lax.optimization_barrier(jnp.sum(wide_rows * wide_rows, axis=1, keepdims=True)) / D + epsilon)
    scaled = (wide_rows * input_norm_gain).astype(jnp.bfloat16)

    def project(weight):
        return (jnp.dot(scaled, weight, preferred_element_type=jnp.float32) * inverse).astype(jnp.bfloat16)
    fresh_input = project(input_matrix)
    fresh_gate = project(gate_matrix)
    fresh_write = project(write_matrix)
    fresh_read = project(read_matrix)
    step_raw = jnp.dot(scaled, step_matrix, preferred_element_type=jnp.float32) * inverse
    next_input = make_window(cached_input_rows, fresh_input, accepted)
    next_write = make_window(cached_write_rows, fresh_write, accepted)
    next_read = make_window(cached_read_rows, fresh_read, accepted)
    conv_input = convolve(next_input, input_kernel).reshape(SEQUENCE_TOTAL, DRAFT_TOKENS, HEAD_TOTAL, P_SIZE)
    conv_write = jnp.repeat(convolve(next_write, write_kernel).reshape(SEQUENCE_TOTAL, DRAFT_TOKENS, G, N), HEAD_TOTAL // G, axis=2)
    conv_read = jnp.repeat(convolve(next_read, read_kernel).reshape(SEQUENCE_TOTAL, DRAFT_TOKENS, G, N), HEAD_TOTAL // G, axis=2)
    step_sizes = jax.nn.softplus(step_raw.reshape(SEQUENCE_TOTAL, DRAFT_TOKENS, HEAD_TOTAL) + step_size_bias)
    retain_logs = -step_sizes * jnp.exp(head_decay_logs) + extra_decay_logs.reshape(SEQUENCE_TOTAL, DRAFT_TOKENS, HEAD_TOTAL)
    carried = cached_state_history[jnp.arange(SEQUENCE_TOTAL, dtype=jnp.int32), accepted]
    states = [carried]
    outputs = []
    for position in range(DRAFT_TOKENS):
        written = (step_sizes[:, position, :, None] * conv_input[:, position])[:, :, :, None]
        carried = jnp.exp(retain_logs[:, position])[:, :, None, None] * carried + written * conv_write[:, position][:, :, None, :]
        states.append(carried)
        outputs.append(lax.optimization_barrier(jnp.sum(carried * conv_read[:, position][:, :, None, :], axis=-1)) + bypass_scale[:, None] * conv_input[:, position])
    head_out = jnp.stack(outputs, axis=1).reshape(TOKENS, HEAD_TOTAL * P_SIZE)
    gated = (head_out * jax.nn.silu(fresh_gate.astype(jnp.float32))).reshape(TOKENS, G, -1)
    gated = gated * lax.rsqrt(lax.optimization_barrier(jnp.mean(gated * gated, axis=-1, keepdims=True)) + epsilon)
    normed = (gated.reshape(TOKENS, HEAD_TOTAL * P_SIZE) * output_norm_gain).astype(jnp.bfloat16)
    span = HEAD_TOTAL * P_SIZE // N_TP
    total = jnp.zeros((TOKENS, D), jnp.float32)
    for block_index in range(N_TP):
        partial_value = jnp.dot(normed[:, block_index * span:(block_index + 1) * span], output_matrix[block_index * span:(block_index + 1) * span], preferred_element_type=jnp.float32)
        total = total + partial_value.astype(jnp.bfloat16).astype(jnp.float32)
    mixer_out = total.astype(jnp.bfloat16)
    next_states = jnp.stack(states, axis=1)
    return (mixer_out, next_states, next_input, next_write, next_read)
```

```python
import functools

import jax
import jax.numpy as jnp
from jax import lax
from jax.experimental import pallas as pl
from jax.experimental.pallas import tpu as pltpu
from jax.sharding import PartitionSpec as P

P_SIZE = 64
N = 128
TAPS = 4
DRAFT_TOKENS = 5
ROWS = DRAFT_TOKENS + TAPS - 1
LEAD = TAPS - 1
MESH = pl.DeviceIdType.MESH
HIGH = lax.Precision.HIGHEST
f32, bf16 = jnp.float32, jnp.bfloat16
epsilon = 1e-05


def factor(count):
    low = max(d for d in range(1, count + 1) if count % d == 0 and d * d <= count)
    return count // low, low


def paired(count):
    return count in (1, 2, 4)


def peer_to(me, d, count):
    if not paired(count):
        return lax.rem(me + d, count)
    if d == count // 2:
        return lax.rem(me + d, count)
    if d == count - 1:
        return count - 1 - me
    return me + 1 - 2 * lax.rem(me, 2)


def peer_from(me, d, count):
    if not paired(count):
        return lax.rem(me - d + count, count)
    return peer_to(me, d, count)


def remote(src, dst, send, recv, where):
    return pltpu.make_async_remote_copy(
        src_ref=src, dst_ref=dst, send_sem=send, recv_sem=recv, device_id=where, device_id_type=MESH
    )


def iota(shape, dim):
    return lax.broadcasted_iota(jnp.int32, shape, dim)


def one_hot(mask):
    return mask.astype(f32).astype(bf16)


def dot(a, b, **more):
    return jnp.dot(a, b, preferred_element_type=f32, **more)


def mixer_kernel(
    nz, ny, nt, own, model_width, plan, group_width,
    tokens_h, gain_h, in_h, gate_h, write_h, read_h, step_h, bias_h, decay_h, extra_h,
    in_taps_h, write_taps_h, read_taps_h, bypass_h, out_gain_h, matrix_h,
    history_h, saved_in_h, saved_write_h, saved_read_h, accepted_h,
    mix, states, next_in, next_write, next_read,
    tokens, gain, w_in, w_gate, w_write, w_read, step_block, bias, decay, extra,
    in_taps, write_taps, read_taps, bypass, out_gain, matrix,
    history, saved_in, saved_write, saved_read, accepted, load_sem,
    wide, ordered, scaled, tail_squares, own_part, tot, tot_own, y_all, keep_all, decay_all,
    step_all, w_all,
    all_a, all_b, rows_b, out_a, out_b, land_a, land_b, final,
    sy, ry, sz, rz, gz_s, gz_r, gy_s, gy_r, st, rt, *rest,
):
    pieces = len(plan)
    send_y, recv_y, send_a, send_b, recv_a, recv_b = [
        rest[i * pieces : (i + 1) * pieces] for i in range(6)
    ]
    me = lax.axis_index("kv")
    col = lax.axis_index("tp")
    z, y = me // ny, lax.rem(me, ny)
    width = w_in.shape[1]
    sw = w_write.shape[1]
    local = tokens.shape[1]
    heads = bias.shape[1]
    seqs = own // DRAFT_TOKENS
    head_rows = own - own % 16
    tail_rows = own - head_rows
    block = nz * own
    full_rows = seqs * ROWS
    pad = tot_own.shape[0]
    groups = width // group_width
    per_group = group_width // P_SIZE

    step_cut = step_h.at[:, pl.ds(pl.multiple_of(me * local, 128), local)]
    pairs = [
        (tokens_h, tokens), (gain_h, gain), (step_cut, step_block), (write_h, w_write),
        (read_h, w_read), (in_h, w_in), (gate_h, w_gate), (bias_h, bias),
        (decay_h, decay), (extra_h, extra), (accepted_h, accepted),
        (saved_in_h, saved_in), (saved_write_h, saved_write), (saved_read_h, saved_read),
        (in_taps_h, in_taps), (write_taps_h, write_taps), (read_taps_h, read_taps),
        (bypass_h, bypass), (out_gain_h, out_gain), (matrix_h, matrix),
    ] + [(history_h.at[s], history.at[s]) for s in range(seqs)]
    loads = [
        pltpu.make_async_copy(source, target, load_sem.at[i])
        for i, (source, target) in enumerate(pairs)
    ]
    for load in loads[:11]:
        load.start()
    y_to = [{"kv": z * ny + lax.rem(y + d, ny)} for d in range(1, ny)]
    z_to = [{"kv": peer_to(z, d, nz) * ny + y} for d in range(1, nz)]
    t_to = [{"tp": peer_to(col, d, nt)} for d in range(1, nt)]
    barrier = pltpu.get_barrier_semaphore()
    for peer in y_to + z_to + t_to:
        pl.semaphore_signal(barrier, inc=1, device_id=peer, device_id_type=MESH)
    for load in loads[11:]:
        load.start()

    loads[0].wait()
    loads[1].wait()
    wide[...] = tokens[...].astype(f32)
    for yy in range(ny):
        for zz in range(nz):
            source = (zz * ny + yy) * own
            at = zz * head_rows
            ordered[yy, at : at + head_rows] = wide[source : source + head_rows]
            if tail_rows:
                at = nz * head_rows + zz * tail_rows
                ordered[yy, at : at + tail_rows] = wide[source + head_rows : source + own]
    lane = iota((block, 128), 1)
    for yy in range(ny):
        values = ordered[yy]
        scaled[yy] = (values * gain[...]).astype(bf16)
        squares = jnp.sum(values * values, axis=1, keepdims=True)
        tail_squares[yy] = jnp.where(lane == heads, squares, 0.0)
    loads[2].wait()
    picked_row = iota((128, step_block.shape[0]), 0)
    pick = (iota((128, step_block.shape[0]), 1) == picked_row + col * heads) & (picked_row < heads)
    picked = dot(one_hot(pick), step_block[...]).astype(bf16)
    loads[3].wait()
    loads[4].wait()
    weights = {"in": w_in, "gate": w_gate}

    def project(kind, first, size, at):
        rows = scaled[at]
        if kind == "small":
            return [
                (0, dot(rows, w_write[...])), (sw, dot(rows, w_read[...])),
                (2 * sw, tail_squares[at] + lax.dot_general(
                    rows, picked, (((1,), (1,)), ((), ())), preferred_element_type=f32
                )),
            ]
        return [(0, dot(rows, weights[kind][:, first : first + size]))]

    y_copies = []
    for p, (kind, first, size) in enumerate(plan):
        if p > 0 and kind == "in" and first == 0:
            loads[5].wait()
        if kind == "gate" and first == 0:
            loads[6].wait()
        copies = []
        for d in range(1, ny):
            for at, part in project(kind, first, size, lax.rem(y + d, ny)):
                send_y[p][d - 1, :, at : at + part.shape[1]] = part.astype(bf16)
            if p == 0 and d == 1:
                pl.semaphore_wait(barrier, len(y_to) + len(z_to) + len(t_to))
            copy = remote(
                send_y[p].at[d - 1], recv_y[p].at[d - 1], sy.at[p, d - 1], ry.at[p, d - 1],
                y_to[d - 1],
            )
            copy.start()
            copies.append(copy)
        y_copies.append(copies)
    if ny == 1:
        pl.semaphore_wait(barrier, len(z_to) + len(t_to))

    offsets = []
    total_columns = 0
    for _, _, size in plan:
        offsets.append(total_columns)
        total_columns += size
    for p, (kind, first, size) in enumerate(plan):
        for at, part in project(kind, first, size, y):
            own_part[:, offsets[p] + at : offsets[p] + at + part.shape[1]] = part
    tot_own[...] = jnp.zeros_like(tot_own)

    z_copies = []
    for p, (_, _, size) in enumerate(plan):
        total = own_part[:, offsets[p] : offsets[p] + size]
        for d in range(1, ny):
            y_copies[p][d - 1].wait_recv()
            total = total + recv_y[p][d - 1].astype(f32)
        tot[:, :size] = total
        for zz in range(nz):
            at = zz * head_rows
            send_a[p][zz] = tot[at : at + head_rows, :size].astype(bf16)
            at = nz * head_rows + zz * tail_rows
            if tail_rows:
                send_b[p][zz] = tot[at : at + tail_rows, :size].astype(bf16)
        copies = []
        for d in reversed(range(1, nz)):
            to = peer_to(z, d, nz)
            for i, (buf, landing) in enumerate(((send_a, recv_a), (send_b, recv_b))):
                if i == 1 and not tail_rows:
                    continue
                copy = remote(
                    buf[p].at[to], landing[p].at[d - 1],
                    sz.at[p, d - 1, i], rz.at[p, d - 1, i], z_to[d - 1],
                )
                copy.start()
                copies.append(copy)
        z_copies.append(copies)

    row = iota((full_rows, pad), 0)
    column = iota((full_rows, pad), 1)
    seq_of, step_of = row // ROWS, lax.rem(row, ROWS)
    token = column - seq_of * DRAFT_TOKENS
    place_tok = one_hot((token == step_of) & (step_of < DRAFT_TOKENS))
    place_win = one_hot((token == step_of - LEAD) & (step_of >= LEAD))
    reach = ((token >= 0) & (token <= step_of) & (token < DRAFT_TOKENS)).astype(f32)
    square_row = iota((full_rows, full_rows), 0)
    square_column = iota((full_rows, full_rows), 1)
    for load in loads[7:19]:
        load.wait()
    taken = [accepted[s] for s in range(seqs)]
    shift = jnp.zeros((full_rows, full_rows), jnp.int32)
    for s in range(seqs):
        shift = jnp.where(square_row // ROWS == s, taken[s], shift)
    picks = one_hot(
        (square_column == square_row + shift) & (lax.rem(square_row, ROWS) < LEAD)
    )

    def gathered(p):
        size = plan[p][2]
        for copy in z_copies[p]:
            copy.wait_recv()
        total_a = send_a[p][z].astype(f32)
        for d in range(1, nz):
            total_a = total_a + recv_a[p][d - 1].astype(f32)
        tot_own[:head_rows, :size] = total_a
        if tail_rows:
            total_b = send_b[p][z].astype(f32)
            for d in range(1, nz):
                total_b = total_b + recv_b[p][d - 1].astype(f32)
            tot_own[head_rows:own, :size] = total_b
        return tot_own[:, :size]

    def convolve(saved, fresh, taps, out):
        kept = saved.astype(f32).reshape(full_rows, saved.shape[2]).astype(bf16)
        window = dot(picks, kept) + dot(place_win, fresh)
        window = window.reshape(seqs, ROWS, saved.shape[2])
        out(window.astype(bf16))
        total = taps[0:1][None] * window
        for k in range(1, TAPS):
            total = total + taps[k : k + 1][None] * pltpu.roll(window, ROWS - k, 1)
        return jax.nn.silu(total).reshape(full_rows, saved.shape[2])

    def store(ref, cut):
        def put(value):
            ref[:, :, cut] = value
        return put

    small = gathered(0)
    tailing = small[:, 2 * sw :]
    inverse = lax.rsqrt(tailing[:, heads : heads + 1] / model_width + epsilon)
    steps = jax.nn.softplus(tailing[:, :heads] * inverse + bias[...])
    fresh = (small[:, : 2 * sw] * inverse).astype(bf16)
    w = convolve(saved_write[...], fresh[:, :sw], write_taps[...], store(next_write, slice(0, sw)))
    r = convolve(saved_read[...], fresh[:, sw:], read_taps[...], store(next_read, slice(0, sw)))
    w_all[...] = w
    added_logs = lax.dot_general(
        (iota((pad, own), 0) == iota((pad, own), 1)).astype(f32), extra[...],
        (((1,), (1,)), ((), ())), precision=HIGH, preferred_element_type=f32,
    )
    logs = jnp.where(iota((pad, heads), 0) < own, -steps * jnp.exp(decay[...]) + added_logs, 0.0)
    summed = dot(reach, logs, precision=HIGH)
    steps_placed = dot(place_tok.astype(f32), steps, precision=HIGH)
    keep_all[...] = jnp.exp(summed)
    spread = (iota((heads, width), 0) == iota((heads, width), 1) // P_SIZE).astype(f32)
    stacked = jnp.concatenate(
        [summed, steps_placed, jnp.broadcast_to(bypass[...], (8, heads))], axis=0
    )
    spreaded = dot(stacked, spread, precision=HIGH)
    decay_all[...] = spreaded[:full_rows]
    step_all[...] = spreaded[full_rows : 2 * full_rows]
    direct = spreaded[2 * full_rows : 2 * full_rows + 1]
    mask_row = iota((ROWS, group_width), 0)
    for load in loads[20:]:
        load.wait()
    p_in = [p for p in range(pieces) if plan[p][0] == "in"]
    p_gate = [p for p in range(pieces) if plan[p][0] == "gate"]
    for g, p in enumerate(p_in):
        cut = slice(g * group_width, (g + 1) * group_width)
        fresh = (gathered(p) * inverse).astype(bf16)
        x = convolve(saved_in[:, :, cut], fresh, in_taps[:, cut], store(next_in, cut))
        step_x = step_all[:, cut] * x
        step_all[:, cut] = step_x
        through = direct[:, cut] * x
        for s in range(seqs):
            rs = slice(s * ROWS, (s + 1) * ROWS)
            wg, rg = w[rs, g * N : (g + 1) * N], r[rs, g * N : (g + 1) * N]
            start = history[s, taken[s], g * per_group : (g + 1) * per_group].reshape(group_width, N)
            out = lax.dot_general(
                rg.astype(bf16), start.astype(bf16), (((1,), (1,)), ((), ())),
                preferred_element_type=f32,
            )
            dg, sg = decay_all[rs, cut], step_x[rs]
            out = out * jnp.exp(dg) + through[rs]
            overlap = lax.dot_general(
                rg, wg, (((1,), (1,)), ((), ())), precision=HIGH, preferred_element_type=f32
            )
            for j in range(DRAFT_TOKENS):
                live = mask_row >= j
                fade = jnp.exp(jnp.where(live, dg - dg[j : j + 1], 0.0))
                out = out + jnp.where(live, fade * overlap[:, j : j + 1] * sg[j : j + 1], 0.0)
            y_all[rs, cut] = out

    def push(g, chunk, sends, recvs, place):
        pair = []
        for i, buf in enumerate((all_a, all_b)):
            if i == 0 or tail_rows:
                pair.append(remote(
                    buf.at[g, chunk], buf.at[g, chunk], sends.at[i], recvs.at[i], place
                ))
                pair[-1].start()
        return pair

    compact_row, compact_column = iota((pad, full_rows), 0), iota((pad, full_rows), 1)
    compact_step = lax.rem(compact_column, ROWS)
    compact = one_hot(
        (compact_row == compact_column // ROWS * DRAFT_TOKENS + compact_step)
        & (compact_step < DRAFT_TOKENS)
    )
    gz_copies, gy_copies = [], []
    for g in range(groups):
        cut = slice(g * group_width, (g + 1) * group_width)
        parts = []
        for p in p_gate:
            if cut.start <= plan[p][1] < cut.stop:
                parts.append(dot(place_tok, (gathered(p) * inverse).astype(bf16)))
        gate = parts[0] if len(parts) == 1 else jnp.concatenate(parts, axis=1)
        gated = y_all[:, cut] * (gate * jax.nn.sigmoid(gate))
        gated = gated * lax.rsqrt(jnp.mean(gated * gated, axis=1, keepdims=True) + epsilon)
        normed = dot(compact, (gated * out_gain[:, cut]).astype(bf16)).astype(bf16)
        all_a[g, me] = normed[:head_rows]
        if tail_rows:
            all_b[g, me] = normed[head_rows:own]
        gz_copies.append([
            push(g, me, gz_s.at[g, d - 1], gz_r.at[g, d - 1], z_to[d - 1])
            for d in reversed(range(1, nz))
        ][::-1])
        gy_copies.append([
            push(g, me, gy_s.at[g, 0, d], gy_r.at[g, 0, d], y_to[d]) for d in range(ny - 1)
        ])

    for s in range(seqs):
        rs = slice(s * ROWS, (s + 1) * ROWS)
        keep = keep_all[rs]
        for g in range(groups):
            cut = slice(g * group_width, (g + 1) * group_width)
            wg, dg, sg = w_all[rs, g * N : (g + 1) * N], decay_all[rs, cut], step_all[rs, cut]
            terms = []
            sides = []
            wide_w = jnp.concatenate([wg] * DRAFT_TOKENS, axis=1)
            wide_lane = iota(wide_w.shape, 1) // N
            for t in range(DRAFT_TOKENS):
                live = mask_row <= t
                fade = jnp.exp(jnp.where(live, dg[t : t + 1] - dg, 0.0))
                terms.append(jnp.where(live, fade * sg, 0.0))
                sides.append(jnp.where(wide_lane == t, wide_w, 0.0))
            left = jnp.concatenate(terms, axis=0).T.astype(bf16)
            added = dot(left, jnp.concatenate(sides, axis=0).astype(bf16))
            for i in range(per_group):
                h = g * per_group + i
                held = history[s, taken[s], h]
                states[s, 0, h] = held
                for t in range(DRAFT_TOKENS):
                    factor_th = jnp.broadcast_to(keep[t : t + 1, h : h + 1], (P_SIZE, N))
                    states[s, t + 1, h] = (
                        factor_th * held
                        + added[i * P_SIZE : (i + 1) * P_SIZE, t * N : (t + 1) * N]
                    )

    for g in range(groups):
        for d in range(1, nz):
            for copy in gz_copies[g][d - 1]:
                copy.wait_recv()
            chunk = peer_from(z, d, nz) * ny + y
            gy_copies[g] += [
                push(g, chunk, gy_s.at[g, d, e], gy_r.at[g, d, e], y_to[e]) for e in range(ny - 1)
            ]
    loads[19].wait()
    part_a, part_b = 0.0, 0.0
    for g in range(groups):
        for pair in gy_copies[g]:
            for copy in pair:
                copy.wait_recv()
        weight = matrix[g * group_width : (g + 1) * group_width]
        part_a = part_a + dot(all_a[g].reshape(nz * ny * head_rows, group_width), weight)
        if tail_rows:
            for k in range(nz * ny):
                rows_b[k * tail_rows : (k + 1) * tail_rows] = all_b[g, k].astype(f32)
            part_b = part_b + dot(rows_b[...].astype(bf16), weight)
    each = nz * ny // nt
    for t in range(nt):
        out_a[t] = part_a[t * each * head_rows : (t + 1) * each * head_rows].astype(bf16)
        if tail_rows:
            out_b[t] = part_b[t * each * tail_rows : (t + 1) * each * tail_rows].astype(bf16)
    t_copies = []
    for d in reversed(range(1, nt)):
        to = peer_to(col, d, nt)
        for i, (buf, landing) in enumerate(((out_a, land_a), (out_b, land_b))):
            if i == 0 or tail_rows:
                copy = remote(
                    buf.at[to], landing.at[d - 1], st.at[d - 1, i], rt.at[d - 1, i], t_to[d - 1]
                )
                copy.start()
                t_copies.append(copy)
    for copy in t_copies:
        copy.wait_recv()
    total_a = out_a[col].astype(f32)
    for d in range(1, nt):
        total_a = total_a + land_a[d - 1].astype(f32)
    if tail_rows:
        total_b = out_b[col].astype(f32)
        for d in range(1, nt):
            total_b = total_b + land_b[d - 1].astype(f32)
    for k in range(each):
        final[k * own : k * own + head_rows] = total_a[k * head_rows : (k + 1) * head_rows]
        if tail_rows:
            final[k * own + head_rows : (k + 1) * own] = (
                total_b[k * tail_rows : (k + 1) * tail_rows]
            )
    mix[...] = final[...].astype(bf16)
    for copies in y_copies + z_copies:
        for copy in copies:
            copy.wait_send()
    for pairs_of in gz_copies + gy_copies:
        for pair in pairs_of:
            for copy in pair:
                copy.wait_send()
    for copy in t_copies:
        copy.wait_send()


def emit_kernel(
    mix, states, next_in, next_write, next_read,
    mix_h, states_h, next_in_h, next_write_h, next_read_h, sem,
):
    pairs = [
        (states.at[s, t], states_h.at[s, t])
        for s in range(states.shape[0]) for t in range(states.shape[1])
    ] + [
        (mix, mix_h), (next_in, next_in_h), (next_write, next_write_h), (next_read, next_read_h),
    ]
    copies = [
        pltpu.make_async_copy(source, target, sem.at[i])
        for i, (source, target) in enumerate(pairs)
    ]
    for copy in copies:
        copy.start()
    for copy in copies:
        copy.wait()


def per_device(
    tokens, input_norm_gain, input_matrix, gate_matrix, write_matrix, read_matrix, step_matrix,
    input_kernel, write_kernel, read_kernel, step_size_bias, head_decay_logs, bypass_scale,
    extra_decay_logs, output_norm_gain, output_matrix, cached_state_history,
    cached_input_rows, cached_write_rows, cached_read_rows, accepted,
):
    kv = lax.axis_size("kv")
    nt = lax.axis_size("tp")
    nz, ny = factor(kv)
    own = tokens.shape[0] // kv
    head_rows = own - own % 16
    tail_rows = max(own - head_rows, 1)
    seqs = own // DRAFT_TOKENS
    full_rows = seqs * ROWS
    pad = -(-own // 16) * 16
    block = nz * own
    local = tokens.shape[1]
    heads = step_size_bias.shape[0]
    width = input_matrix.shape[1]
    sw = write_matrix.shape[1]
    group_width = width // (sw // N)
    groups = width // group_width
    half = group_width // 2
    out_width = output_matrix.shape[1]
    each = kv // nt
    vmem = pl.BlockSpec(memory_space=pltpu.VMEM)
    hbm = pl.BlockSpec(memory_space=pltpu.HBM)
    plan = [("small", 0, 2 * sw + 128)]
    plan += [("in", g * group_width, group_width) for g in range(groups)]
    plan += [("gate", g * group_width, group_width) for g in range(groups - 1)]
    last = (groups - 1) * group_width
    plan += [("gate", last, half), ("gate", last + half, half)]
    sizes = [size for _, _, size in plan]
    pieces = len(plan)
    dma = pltpu.SemaphoreType.DMA
    peers = max(ny - 1, 1)
    shape = jax.ShapeDtypeStruct
    operands = (
        tokens, input_norm_gain[None], input_matrix, gate_matrix, write_matrix, read_matrix,
        step_matrix.T, step_size_bias[None], head_decay_logs[None], extra_decay_logs.T,
        input_kernel, write_kernel, read_kernel, bypass_scale[None], output_norm_gain[None],
        output_matrix, cached_state_history, cached_input_rows, cached_write_rows,
        cached_read_rows, accepted,
    )
    step_shape = (step_matrix.shape[1], local)
    buffers = [
        pltpu.VMEM(step_shape if i == 6 else a.shape, a.dtype)
        for i, a in enumerate(operands[:-1])
    ]
    results = (
        ((each * own, out_width), bf16), (cached_state_history.shape, f32),
        (cached_input_rows.shape, bf16), (cached_write_rows.shape, bf16),
        (cached_read_rows.shape, bf16),
    )
    outs = pl.pallas_call(
        functools.partial(
            mixer_kernel, nz, ny, nt, own, local * kv, tuple(plan), group_width
        ),
        out_shape=tuple(pltpu.VMEM(dims, kind) for dims, kind in results),
        in_specs=[hbm] * len(operands),
        out_specs=[vmem] * len(results),
        scratch_shapes=buffers + [
            pltpu.SMEM(accepted.shape, jnp.int32),
            dma((len(operands) - 1 + seqs,)),
            pltpu.VMEM(tokens.shape, f32),
            pltpu.VMEM((ny, block, local), f32),
            pltpu.VMEM((ny, block, local), bf16),
            pltpu.VMEM((ny, block, 128), f32),
            pltpu.VMEM((block, sum(sizes)), f32),
            pltpu.VMEM((block, max(sizes)), f32),
            pltpu.VMEM((pad, max(sizes)), f32),
            pltpu.VMEM((full_rows, width), f32),
            pltpu.VMEM((full_rows, heads), f32),
            pltpu.VMEM((full_rows, width), f32),
            pltpu.VMEM((full_rows, width), f32),
            pltpu.VMEM((full_rows, sw), f32),
            pltpu.VMEM((groups, kv, head_rows, group_width), bf16),
            pltpu.VMEM((groups, kv, tail_rows, group_width), bf16),
            pltpu.VMEM((kv * tail_rows, group_width), f32),
            pltpu.VMEM((nt, each * head_rows, out_width), bf16),
            pltpu.VMEM((nt, each * tail_rows, out_width), bf16),
            pltpu.VMEM((nt - 1, each * head_rows, out_width), bf16),
            pltpu.VMEM((nt - 1, each * tail_rows, out_width), bf16),
            pltpu.VMEM((each * own, out_width), f32),
            dma((pieces, peers)), dma((pieces, peers)),
            dma((pieces, nz - 1, 2)), dma((pieces, nz - 1, 2)),
            dma((groups, nz - 1, 2)), dma((groups, nz - 1, 2)),
            dma((groups, nz, peers, 2)), dma((groups, nz, peers, 2)),
            dma((nt - 1, 2)), dma((nt - 1, 2)),
        ]
        + [pltpu.VMEM((peers, block, c), bf16) for c in sizes]
        + [pltpu.VMEM((peers, block, c), bf16) for c in sizes]
        + [pltpu.VMEM((nz, head_rows, c), bf16) for c in sizes]
        + [pltpu.VMEM((nz, tail_rows, c), bf16) for c in sizes]
        + [pltpu.VMEM((nz - 1, head_rows, c), bf16) for c in sizes]
        + [pltpu.VMEM((nz - 1, tail_rows, c), bf16) for c in sizes],
        compiler_params=pltpu.CompilerParams(
            collective_id=0, has_side_effects=True, vmem_limit_bytes=40 * 2**20
        ),
    )(*[pltpu.with_memory_space_constraint(a, pltpu.HBM) for a in operands])
    return tuple(pl.pallas_call(
        emit_kernel,
        out_shape=tuple(shape(dims, kind) for dims, kind in results),
        in_specs=[vmem] * len(results),
        out_specs=[hbm] * len(results),
        scratch_shapes=[dma((seqs * (DRAFT_TOKENS + 1) + len(results) - 1,))],
        compiler_params=pltpu.CompilerParams(vmem_limit_bytes=2**20),
    )(*outs))


def solution(mesh):
    return jax.shard_map(
        per_device,
        mesh=mesh,
        in_specs=(
            P(None, "kv"),
            P("kv"),
            P("kv", "tp"),
            P("kv", "tp"),
            P("kv", "tp"),
            P("kv", "tp"),
            P(),
            P(None, "tp"),
            P(None, "tp"),
            P(None, "tp"),
            P("tp"),
            P("tp"),
            P("tp"),
            P("kv", "tp"),
            P("tp"),
            P("tp", "kv"),
            P("kv", None, "tp", None, None),
            P("kv", None, "tp"),
            P("kv", None, "tp"),
            P("kv", None, "tp"),
            P("kv"),
        ),
        out_specs=(
            P("tp", "kv"),
            P("kv", None, "tp", None, None),
            P("kv", None, "tp"),
            P("kv", None, "tp"),
            P("kv", None, "tp"),
        ),
        check_vma=False,
    )
```

```python
import functools

import jax
import jax.numpy as jnp
from jax import lax
from jax.experimental import pallas as pl
from jax.experimental.pallas import tpu as pltpu
from jax.sharding import PartitionSpec as P

P_SIZE = 64
N = 128
TAPS = 4
DRAFT_TOKENS = 5
ROWS = DRAFT_TOKENS + TAPS - 1
LEAD = TAPS - 1
MESH = pl.DeviceIdType.MESH
HIGH = lax.Precision.HIGHEST
f32, bf16 = jnp.float32, jnp.bfloat16
epsilon = 1e-05


def factor(count):
    low = max(d for d in range(1, count + 1) if count % d == 0 and d * d <= count)
    return count // low, low


def paired(count):
    return count in (1, 2, 4)


def peer_to(me, d, count):
    if d == 0:
        return me
    if not paired(count):
        return lax.rem(me + d, count)
    if d == count // 2:
        return lax.rem(me + d, count)
    if d == count - 1:
        return count - 1 - me
    return me + 1 - 2 * lax.rem(me, 2)


def static_to(me, d, count):
    return me ^ d if paired(count) else (me + d) % count


def peer_from(me, d, count):
    if not paired(count):
        return lax.rem(me - d + count, count)
    return peer_to(me, d, count)


def remote(src, dst, send, recv, where):
    return pltpu.make_async_remote_copy(
        src_ref=src, dst_ref=dst, send_sem=send, recv_sem=recv, device_id=where, device_id_type=MESH
    )


def iota(shape, dim):
    return lax.broadcasted_iota(jnp.int32, shape, dim)


def one_hot(mask):
    return mask.astype(f32).astype(bf16)


def dot(a, b, **more):
    return jnp.dot(a, b, preferred_element_type=f32, **more)


def mixer_kernel(
    nz, ny, nt, own, model_width, plan, group_width,
    tokens_h, gain_h, in_h, gate_h, write_h, read_h, step_h, bias_h, decay_h, extra_h,
    in_taps_h, write_taps_h, read_taps_h, bypass_h, out_gain_h, matrix_h,
    history_h, saved_in_h, saved_write_h, saved_read_h, accepted_h,
    mix, *more,
):
    away, more = more[: nt - 1], more[nt - 1 :]
    (states, next_in, next_write, next_read), more = more[:4], more[4:]
    (
    tokens, gain, w_in, w_gate, w_write, w_read, step_block, bias, decay, extra,
    in_taps, write_taps, read_taps, bypass, out_gain, matrix,
    history, saved_in, saved_write, saved_read, accepted, load_sem,
    wide, ordered, scaled, tail_squares, own_part, tot, tot_own, y_all, keep_all, decay_all,
    step_all, w_all,
    all_a, all_b, rows_b, final,
    sy, ry, sz, rz, gz_s, gz_r, gy_s, gy_r, *rest,
    ) = more
    pieces = len(plan)
    send_y, recv_y, send_a, send_b, recv_a, recv_b = [
        rest[i * pieces : (i + 1) * pieces] for i in range(6)
    ]
    me = lax.axis_index("kv")
    col = lax.axis_index("tp")
    z, y = me // ny, lax.rem(me, ny)
    width = w_in.shape[1]
    sw = w_write.shape[1]
    local = tokens.shape[1]
    heads = bias.shape[1]
    seqs = own // DRAFT_TOKENS
    head_rows = own - own % 16
    tail_rows = own - head_rows
    block = nz * own
    full_rows = seqs * ROWS
    pad = tot_own.shape[0]
    groups = width // group_width
    per_group = group_width // P_SIZE

    step_cut = step_h.at[:, pl.ds(pl.multiple_of(me * local, 128), local)]
    pairs = [
        (tokens_h, tokens), (gain_h, gain), (step_cut, step_block), (write_h, w_write),
        (read_h, w_read), (in_h, w_in), (gate_h, w_gate), (bias_h, bias),
        (decay_h, decay), (extra_h, extra), (accepted_h, accepted),
        (saved_in_h, saved_in), (saved_write_h, saved_write), (saved_read_h, saved_read),
        (in_taps_h, in_taps), (write_taps_h, write_taps), (read_taps_h, read_taps),
        (bypass_h, bypass), (out_gain_h, out_gain), (matrix_h, matrix),
    ] + [(history_h.at[s], history.at[s]) for s in range(seqs)]
    loads = [
        pltpu.make_async_copy(source, target, load_sem.at[i])
        for i, (source, target) in enumerate(pairs)
    ]
    for load in loads[:11]:
        load.start()
    y_to = [{"kv": z * ny + lax.rem(y + d, ny)} for d in range(1, ny)]
    z_to = [{"kv": peer_to(z, d, nz) * ny + y} for d in range(1, nz)]
    cross = [
        [{"kv": peer_to(z, d, nz) * ny + lax.rem(y + e, ny)} for e in range(1, ny)]
        for d in range(1, nz)
    ]
    barrier = pltpu.get_barrier_semaphore()
    everyone = y_to + z_to + sum(cross, [])
    for peer in everyone:
        pl.semaphore_signal(barrier, inc=1, device_id=peer, device_id_type=MESH)
    for load in loads[11:]:
        load.start()

    loads[0].wait()
    loads[1].wait()
    wide[...] = tokens[...].astype(f32)
    for yy in range(ny):
        for zz in range(nz):
            source = (zz * ny + yy) * own
            at = zz * head_rows
            ordered[yy, at : at + head_rows] = wide[source : source + head_rows]
            if tail_rows:
                at = nz * head_rows + zz * tail_rows
                ordered[yy, at : at + tail_rows] = wide[source + head_rows : source + own]
    lane = iota((block, 128), 1)
    for yy in range(ny):
        values = ordered[yy]
        scaled[yy] = (values * gain[...]).astype(bf16)
        squares = jnp.sum(values * values, axis=1, keepdims=True)
        tail_squares[yy] = jnp.where(lane == heads, squares, 0.0)
    loads[2].wait()
    picked_row = iota((128, step_block.shape[0]), 0)
    pick = (iota((128, step_block.shape[0]), 1) == picked_row + col * heads) & (picked_row < heads)
    picked = dot(one_hot(pick), step_block[...]).astype(bf16)
    loads[3].wait()
    weights = {"read": w_read, "in": w_in, "gate": w_gate}

    def project(kind, first, size, at):
        rows = scaled[at]
        if kind == "write":
            return [
                (0, dot(rows, w_write[...])),
                (sw, tail_squares[at] + lax.dot_general(
                    rows, picked, (((1,), (1,)), ((), ())), preferred_element_type=f32
                )),
            ]
        return [(0, dot(rows, weights[kind][:, first : first + size]))]

    y_copies = []
    for p, (kind, first, size) in enumerate(plan):
        if first == 0 and kind in ("read", "in", "gate"):
            loads[{"read": 4, "in": 5, "gate": 6}[kind]].wait()
        copies = []
        for d in range(1, ny):
            for at, part in project(kind, first, size, lax.rem(y + d, ny)):
                send_y[p][d - 1, :, at : at + part.shape[1]] = part.astype(bf16)
            if p == 0 and d == 1:
                pl.semaphore_wait(barrier, len(everyone))
            copy = remote(
                send_y[p].at[d - 1], recv_y[p].at[d - 1], sy.at[p, d - 1], ry.at[p, d - 1],
                y_to[d - 1],
            )
            copy.start()
            copies.append(copy)
        y_copies.append(copies)
    if ny == 1:
        pl.semaphore_wait(barrier, len(everyone))

    offsets = []
    total_columns = 0
    for _, _, size in plan:
        offsets.append(total_columns)
        total_columns += size
    for p, (kind, first, size) in enumerate(plan):
        for at, part in project(kind, first, size, y):
            own_part[:, offsets[p] + at : offsets[p] + at + part.shape[1]] = part
    tot_own[...] = jnp.zeros_like(tot_own)
    y_all[...] = jnp.zeros_like(y_all)

    z_copies = []
    for p, (_, _, size) in enumerate(plan):
        total = own_part[:, offsets[p] : offsets[p] + size]
        for d in range(1, ny):
            y_copies[p][d - 1].wait_recv()
            total = total + recv_y[p][d - 1].astype(f32)
        tot[:, :size] = total
        for zz in range(nz):
            at = zz * head_rows
            send_a[p][zz] = tot[at : at + head_rows, :size].astype(bf16)
            at = nz * head_rows + zz * tail_rows
            if tail_rows:
                send_b[p][zz] = tot[at : at + tail_rows, :size].astype(bf16)
        copies = []
        for d in reversed(range(1, nz)):
            to = peer_to(z, d, nz)
            for i, (buf, landing) in enumerate(((send_a, recv_a), (send_b, recv_b))):
                if i == 1 and not tail_rows:
                    continue
                copy = remote(
                    buf[p].at[to], landing[p].at[d - 1],
                    sz.at[p, d - 1, i], rz.at[p, d - 1, i], z_to[d - 1],
                )
                copy.start()
                copies.append(copy)
        z_copies.append(copies)

    row = iota((full_rows, pad), 0)
    column = iota((full_rows, pad), 1)
    seq_of, step_of = row // ROWS, lax.rem(row, ROWS)
    token = column - seq_of * DRAFT_TOKENS
    place_tok = one_hot((token == step_of) & (step_of < DRAFT_TOKENS))
    place_win = one_hot((token == step_of - LEAD) & (step_of >= LEAD))
    reach = ((token >= 0) & (token <= step_of) & (token < DRAFT_TOKENS)).astype(f32)
    square_row = iota((full_rows, full_rows), 0)
    square_column = iota((full_rows, full_rows), 1)
    for load in loads[7:19]:
        load.wait()
    taken = [accepted[s] for s in range(seqs)]
    shift = jnp.zeros((full_rows, full_rows), jnp.int32)
    for s in range(seqs):
        shift = jnp.where(square_row // ROWS == s, taken[s], shift)
    picks = one_hot(
        (square_column == square_row + shift) & (lax.rem(square_row, ROWS) < LEAD)
    )

    def gathered(p):
        size = plan[p][2]
        for copy in z_copies[p]:
            copy.wait_recv()
        total_a = send_a[p][z].astype(f32)
        for d in range(1, nz):
            total_a = total_a + recv_a[p][d - 1].astype(f32)
        tot_own[:head_rows, :size] = total_a
        if tail_rows:
            total_b = send_b[p][z].astype(f32)
            for d in range(1, nz):
                total_b = total_b + recv_b[p][d - 1].astype(f32)
            tot_own[head_rows:own, :size] = total_b
        return tot_own[:, :size]

    def convolve(saved, fresh, taps, out):
        kept = saved.astype(f32).reshape(full_rows, saved.shape[2]).astype(bf16)
        window = dot(picks, kept) + dot(place_win, fresh)
        window = window.reshape(seqs, ROWS, saved.shape[2])
        out(window.astype(bf16))
        total = taps[0:1][None] * window
        for k in range(1, TAPS):
            total = total + taps[k : k + 1][None] * pltpu.roll(window, ROWS - k, 1)
        return jax.nn.silu(total).reshape(full_rows, saved.shape[2])

    def store(ref, cut):
        def put(value):
            ref[:, :, cut] = value
        return put

    small = gathered(0)
    tailing = small[:, sw:]
    inverse = lax.rsqrt(tailing[:, heads : heads + 1] / model_width + epsilon)
    steps = jax.nn.softplus(tailing[:, :heads] * inverse + bias[...])
    fresh = (small[:, :sw] * inverse).astype(bf16)
    w = convolve(saved_write[...], fresh, write_taps[...], store(next_write, slice(0, sw)))
    fresh = (gathered(1) * inverse).astype(bf16)
    r = convolve(saved_read[...], fresh, read_taps[...], store(next_read, slice(0, sw)))
    w_all[...] = w
    added_logs = lax.dot_general(
        (iota((pad, own), 0) == iota((pad, own), 1)).astype(f32), extra[...],
        (((1,), (1,)), ((), ())), precision=HIGH, preferred_element_type=f32,
    )
    logs = jnp.where(iota((pad, heads), 0) < own, -steps * jnp.exp(decay[...]) + added_logs, 0.0)
    summed = dot(reach, logs, precision=HIGH)
    steps_placed = dot(place_tok.astype(f32), steps, precision=HIGH)
    keep_all[...] = jnp.exp(summed)
    spread = (iota((heads, width), 0) == iota((heads, width), 1) // P_SIZE).astype(f32)
    stacked = jnp.concatenate(
        [summed, steps_placed, jnp.broadcast_to(bypass[...], (8, heads))], axis=0
    )
    spreaded = dot(stacked, spread, precision=HIGH)
    decay_all[...] = spreaded[:full_rows]
    step_all[...] = spreaded[full_rows : 2 * full_rows]
    direct = spreaded[2 * full_rows : 2 * full_rows + 1]
    mask_row = iota((ROWS, group_width), 0)
    for load in loads[20:]:
        load.wait()
    p_in = [p for p in range(pieces) if plan[p][0] == "in"]
    p_gate = [p for p in range(pieces) if plan[p][0] == "gate"]
    for g, p in enumerate(p_in):
        cut = slice(g * group_width, (g + 1) * group_width)
        fresh = (gathered(p) * inverse).astype(bf16)
        x = convolve(saved_in[:, :, cut], fresh, in_taps[:, cut], store(next_in, cut))
        step_x = step_all[:, cut] * x
        step_all[:, cut] = step_x
        through = direct[:, cut] * x
        for s in range(seqs):
            rs = slice(s * ROWS, (s + 1) * ROWS)
            wg, rg = w[rs, g * N : (g + 1) * N], r[rs, g * N : (g + 1) * N]
            start = history[s, taken[s], g * per_group : (g + 1) * per_group].reshape(group_width, N)
            out = lax.dot_general(
                rg.astype(bf16), start.astype(bf16), (((1,), (1,)), ((), ())),
                preferred_element_type=f32,
            )
            dg, sg = decay_all[rs, cut], step_x[rs]
            out = out * jnp.exp(dg) + through[rs]
            overlap = lax.dot_general(
                rg, wg, (((1,), (1,)), ((), ())), precision=HIGH, preferred_element_type=f32
            )
            for j in range(DRAFT_TOKENS):
                live = mask_row >= j
                fade = jnp.exp(jnp.where(live, dg - dg[j : j + 1], 0.0))
                out = out + jnp.where(live, fade * overlap[:, j : j + 1] * sg[j : j + 1], 0.0)
            y_all[s * DRAFT_TOKENS : (s + 1) * DRAFT_TOKENS, cut] = out[:DRAFT_TOKENS]

    def push(g, chunk, sends, recvs, place):
        pair = []
        for i, buf in enumerate((all_a, all_b)):
            if i == 0 or tail_rows:
                pair.append(remote(
                    buf.at[g, chunk], buf.at[g, chunk], sends.at[i], recvs.at[i], place
                ))
                pair[-1].start()
        return pair

    gz_copies, gy_copies = [], []
    for g in range(groups):
        cut = slice(g * group_width, (g + 1) * group_width)
        parts = []
        for p in p_gate:
            if cut.start <= plan[p][1] < cut.stop:
                parts.append((gathered(p) * inverse).astype(bf16).astype(f32))
        gate = parts[0] if len(parts) == 1 else jnp.concatenate(parts, axis=1)
        gated = y_all[:, cut] * (gate * jax.nn.sigmoid(gate))
        gated = gated * lax.rsqrt(jnp.mean(gated * gated, axis=1, keepdims=True) + epsilon)
        normed = (gated * out_gain[:, cut]).astype(bf16)
        all_a[g, me] = normed[:head_rows]
        if tail_rows:
            all_b[g, me] = normed[head_rows:own]
        gz_copies.append([])
        gy_copies.append([])
        for d in reversed(range(1, nz)):
            gz_copies[g].insert(
                0, push(g, me, gz_s.at[g, d - 1], gz_r.at[g, d - 1], z_to[d - 1])
            )
            if g == groups - 1:
                gy_copies[g] += [
                    push(g, me, gy_s.at[g, d, e], gy_r.at[g, d, e], cross[d - 1][e])
                    for e in range(ny - 1)
                ]
        gy_copies[g] += [
            push(g, me, gy_s.at[g, 0, e], gy_r.at[g, 0, e], y_to[e]) for e in range(ny - 1)
        ]

    for s in range(seqs):
        rs = slice(s * ROWS, (s + 1) * ROWS)
        keep = keep_all[rs]
        for g in range(groups):
            cut = slice(g * group_width, (g + 1) * group_width)
            wg, dg, sg = w_all[rs, g * N : (g + 1) * N], decay_all[rs, cut], step_all[rs, cut]
            terms = []
            sides = []
            wide_w = jnp.concatenate([wg] * DRAFT_TOKENS, axis=1)
            wide_lane = iota(wide_w.shape, 1) // N
            for t in range(DRAFT_TOKENS):
                live = mask_row <= t
                fade = jnp.exp(jnp.where(live, dg[t : t + 1] - dg, 0.0))
                terms.append(jnp.where(live, fade * sg, 0.0))
                sides.append(jnp.where(wide_lane == t, wide_w, 0.0))
            left = jnp.concatenate(terms, axis=0).T.astype(bf16)
            added = dot(left, jnp.concatenate(sides, axis=0).astype(bf16))
            for i in range(per_group):
                h = g * per_group + i
                held = history[s, taken[s], h]
                states[s, 0, h] = held
                for t in range(DRAFT_TOKENS):
                    factor_th = jnp.broadcast_to(keep[t : t + 1, h : h + 1], (P_SIZE, N))
                    states[s, t + 1, h] = (
                        factor_th * held
                        + added[i * P_SIZE : (i + 1) * P_SIZE, t * N : (t + 1) * N]
                    )

    for g in range(groups):
        for d in range(1, nz):
            for copy in gz_copies[g][d - 1]:
                copy.wait_recv()
            if g < groups - 1:
                chunk = peer_from(z, d, nz) * ny + y
                gy_copies[g] += [
                    push(g, chunk, gy_s.at[g, d, e], gy_r.at[g, d, e], y_to[e])
                    for e in range(ny - 1)
                ]
    loads[19].wait()
    for g in range(groups):
        for pair in gy_copies[g]:
            for copy in pair:
                copy.wait_recv()
        for k in range(nz * ny):
            if tail_rows:
                rows_b[g, k * tail_rows : (k + 1) * tail_rows] = all_b[g, k].astype(f32)
    each = nz * ny // nt

    span = nz * ny * head_rows
    product = 0.0
    for g in range(groups):
        left = all_a[g].reshape(span, group_width)
        if tail_rows:
            left = jnp.concatenate([left, rows_b[g].astype(bf16)], axis=0)
        product = product + dot(left, matrix[g * group_width : (g + 1) * group_width])
    for t in range(nt):
        for k in range(each):
            at = (t * each + k) * head_rows
            final[t, k * own : k * own + head_rows] = product[at : at + head_rows]
            if tail_rows:
                at = span + (t * each + k) * tail_rows
                final[t, k * own + head_rows : (k + 1) * own] = product[at : at + tail_rows]
    for d in reversed(range(1, nt)):
        away[d - 1][...] = final[peer_to(col, d, nt)].astype(bf16)
    mix[...] = final[col]
    for copies in y_copies + z_copies:
        for copy in copies:
            copy.wait_send()
    for pairs_of in gz_copies + gy_copies:
        for pair in pairs_of:
            for copy in pair:
                copy.wait_send()


def emit_kernel(
    states, next_in, next_write, next_read,
    states_h, next_in_h, next_write_h, next_read_h, sem,
):
    pairs = [
        (states.at[s, t], states_h.at[s, t])
        for s in range(states.shape[0]) for t in range(states.shape[1])
    ] + [
        (next_in, next_in_h), (next_write, next_write_h), (next_read, next_read_h),
    ]
    copies = [
        pltpu.make_async_copy(source, target, sem.at[i])
        for i, (source, target) in enumerate(pairs)
    ]
    for copy in copies:
        copy.start()
    for copy in copies:
        copy.wait()


def per_device(
    tokens, input_norm_gain, input_matrix, gate_matrix, write_matrix, read_matrix, step_matrix,
    input_kernel, write_kernel, read_kernel, step_size_bias, head_decay_logs, bypass_scale,
    extra_decay_logs, output_norm_gain, output_matrix, cached_state_history,
    cached_input_rows, cached_write_rows, cached_read_rows, accepted,
):
    kv = lax.axis_size("kv")
    nt = lax.axis_size("tp")
    nz, ny = factor(kv)
    own = tokens.shape[0] // kv
    head_rows = own - own % 16
    tail_rows = max(own - head_rows, 1)
    seqs = own // DRAFT_TOKENS
    full_rows = seqs * ROWS
    pad = -(-own // 16) * 16
    block = nz * own
    local = tokens.shape[1]
    heads = step_size_bias.shape[0]
    width = input_matrix.shape[1]
    sw = write_matrix.shape[1]
    group_width = width // (sw // N)
    groups = width // group_width
    half = group_width // 2
    out_width = output_matrix.shape[1]
    each = kv // nt
    vmem = pl.BlockSpec(memory_space=pltpu.VMEM)
    hbm = pl.BlockSpec(memory_space=pltpu.HBM)
    plan = [("write", 0, sw + 128), ("read", 0, sw)]
    plan += [("in", g * group_width, group_width) for g in range(groups)]
    plan += [("gate", g * group_width, group_width) for g in range(groups - 1)]
    last = (groups - 1) * group_width
    quarter = half // 2
    plan += [
        ("gate", last, half), ("gate", last + half, half),
    ]
    sizes = [size for _, _, size in plan]
    pieces = len(plan)
    dma = pltpu.SemaphoreType.DMA
    peers = max(ny - 1, 1)
    shape = jax.ShapeDtypeStruct
    operands = (
        tokens, input_norm_gain[None], input_matrix, gate_matrix, write_matrix, read_matrix,
        step_matrix.T, step_size_bias[None], head_decay_logs[None], extra_decay_logs.T,
        input_kernel, write_kernel, read_kernel, bypass_scale[None], output_norm_gain[None],
        output_matrix, cached_state_history, cached_input_rows, cached_write_rows,
        cached_read_rows, accepted,
    )
    step_shape = (step_matrix.shape[1], local)
    buffers = [
        pltpu.VMEM(step_shape if i == 6 else a.shape, a.dtype)
        for i, a in enumerate(operands[:-1])
    ]
    part = (each * own, out_width)
    results = (
        (cached_state_history.shape, f32), (cached_input_rows.shape, bf16),
        (cached_write_rows.shape, bf16), (cached_read_rows.shape, bf16),
    )
    everything = ((part, f32),) + ((part, bf16),) * (nt - 1) + results
    outs = pl.pallas_call(
        functools.partial(
            mixer_kernel, nz, ny, nt, own, local * kv, tuple(plan), group_width
        ),
        out_shape=tuple(pltpu.VMEM(dims, kind) for dims, kind in everything),
        in_specs=[hbm] * len(operands),
        out_specs=[vmem] * len(everything),
        scratch_shapes=buffers + [
            pltpu.SMEM(accepted.shape, jnp.int32),
            dma((len(operands) - 1 + seqs,)),
            pltpu.VMEM(tokens.shape, f32),
            pltpu.VMEM((ny, block, local), f32),
            pltpu.VMEM((ny, block, local), bf16),
            pltpu.VMEM((ny, block, 128), f32),
            pltpu.VMEM((block, sum(sizes)), f32),
            pltpu.VMEM((block, max(sizes)), f32),
            pltpu.VMEM((pad, max(sizes)), f32),
            pltpu.VMEM((pad, width), f32),
            pltpu.VMEM((full_rows, heads), f32),
            pltpu.VMEM((full_rows, width), f32),
            pltpu.VMEM((full_rows, width), f32),
            pltpu.VMEM((full_rows, sw), f32),
            pltpu.VMEM((groups, kv, head_rows, group_width), bf16),
            pltpu.VMEM((groups, kv, tail_rows, group_width), bf16),
            pltpu.VMEM((groups, kv * tail_rows, group_width), f32),
            pltpu.VMEM((nt, each * own, out_width), f32),
            dma((pieces, peers)), dma((pieces, peers)),
            dma((pieces, nz - 1, 2)), dma((pieces, nz - 1, 2)),
            dma((groups, nz - 1, 2)), dma((groups, nz - 1, 2)),
            dma((groups, nz, peers, 2)), dma((groups, nz, peers, 2)),
        ]
        + [pltpu.VMEM((peers, block, c), bf16) for c in sizes]
        + [pltpu.VMEM((peers, block, c), bf16) for c in sizes]
        + [pltpu.VMEM((nz, head_rows, c), bf16) for c in sizes]
        + [pltpu.VMEM((nz, tail_rows, c), bf16) for c in sizes]
        + [pltpu.VMEM((nz - 1, head_rows, c), bf16) for c in sizes]
        + [pltpu.VMEM((nz - 1, tail_rows, c), bf16) for c in sizes],
        compiler_params=pltpu.CompilerParams(
            collective_id=0, has_side_effects=True, vmem_limit_bytes=40 * 2**20
        ),
    )(*[pltpu.with_memory_space_constraint(a, pltpu.HBM) for a in operands])
    kept = pl.pallas_call(
        emit_kernel,
        out_shape=tuple(shape(dims, kind) for dims, kind in results),
        in_specs=[vmem] * len(results),
        out_specs=[hbm] * len(results),
        scratch_shapes=[dma((seqs * (DRAFT_TOKENS + 1) + len(results) - 1,))],
        compiler_params=pltpu.CompilerParams(vmem_limit_bytes=2**20),
        cost_estimate=pl.CostEstimate(flops=10**8, bytes_accessed=10**7, transcendentals=0),
    )(*outs[nt:])
    total = outs[0]
    for d in range(1, nt):
        ring = [(i, static_to(i, d, nt)) for i in range(nt)]
        total = total + lax.ppermute(outs[d], "tp", ring).astype(f32)
    return (total.astype(bf16),) + tuple(kept)


def solution(mesh):
    return jax.shard_map(
        per_device,
        mesh=mesh,
        in_specs=(
            P(None, "kv"),
            P("kv"),
            P("kv", "tp"),
            P("kv", "tp"),
            P("kv", "tp"),
            P("kv", "tp"),
            P(),
            P(None, "tp"),
            P(None, "tp"),
            P(None, "tp"),
            P("tp"),
            P("tp"),
            P("tp"),
            P("kv", "tp"),
            P("tp"),
            P("tp", "kv"),
            P("kv", None, "tp", None, None),
            P("kv", None, "tp"),
            P("kv", None, "tp"),
            P("kv", None, "tp"),
            P("kv"),
        ),
        out_specs=(
            P("tp", "kv"),
            P("kv", None, "tp", None, None),
            P("kv", None, "tp"),
            P("kv", None, "tp"),
            P("kv", None, "tp"),
        ),
        check_vma=False,
    )
```

```python
import functools

import jax
import jax.numpy as jnp
from jax import lax
from jax.experimental import pallas as pl
from jax.experimental.pallas import tpu as pltpu
from jax.sharding import PartitionSpec as P

P_SIZE = 64
N = 128
TAPS = 4
DRAFT_TOKENS = 5
ROWS = DRAFT_TOKENS + TAPS - 1
LEAD = TAPS - 1
MESH = pl.DeviceIdType.MESH
HIGH = lax.Precision.HIGHEST
f32, bf16 = jnp.float32, jnp.bfloat16
epsilon = 1e-05


def factor(count):
    low = max(d for d in range(1, count + 1) if count % d == 0 and d * d <= count)
    return count // low, low


def paired(count):
    return count in (1, 2, 4)


def peer_to(me, d, count):
    if d == 0:
        return me
    if not paired(count):
        return lax.rem(me + d, count)
    if d == count // 2:
        return lax.rem(me + d, count)
    if d == count - 1:
        return count - 1 - me
    return me + 1 - 2 * lax.rem(me, 2)


def static_to(me, d, count):
    return me ^ d if paired(count) else (me + d) % count


def peer_from(me, d, count):
    if not paired(count):
        return lax.rem(me - d + count, count)
    return peer_to(me, d, count)


def remote(src, dst, send, recv, where):
    return pltpu.make_async_remote_copy(
        src_ref=src, dst_ref=dst, send_sem=send, recv_sem=recv, device_id=where, device_id_type=MESH
    )


def iota(shape, dim):
    return lax.broadcasted_iota(jnp.int32, shape, dim)


def one_hot(mask):
    return mask.astype(f32).astype(bf16)


def dot(a, b, **more):
    return jnp.dot(a, b, preferred_element_type=f32, **more)


def mixer_kernel(
    nz, ny, nt, own, model_width, plan, group_width,
    tokens_h, gain_h, in_h, gate_h, write_h, read_h, step_h, bias_h, decay_h, extra_h,
    in_taps_h, write_taps_h, read_taps_h, bypass_h, out_gain_h, matrix_h,
    history_h, saved_in_h, saved_write_h, saved_read_h, accepted_h,
    mix, *more,
):
    away, more = more[: nt - 1], more[nt - 1 :]
    (states, next_in, next_write, next_read), more = more[:4], more[4:]
    (
    tokens, gain, w_in, w_gate, w_write, w_read, step_block, bias, decay, extra,
    in_taps, write_taps, read_taps, bypass, out_gain, matrix,
    history, saved_in, saved_write, saved_read, accepted, load_sem,
    wide, ordered, scaled, tail_squares, own_part, tot, tot_own, y_all, keep_all, decay_all,
    step_all, w_all,
    all_a, all_b, rows_b, final,
    sy, ry, sz, rz, gz_s, gz_r, gy_s, gy_r,
    ez_send_a, ez_send_b, ez_recv_a, ez_recv_b, ey_send_a, ey_send_b, ey_recv_a, ey_recv_b,
    ez_s, ez_r, ey_s, ey_r, *rest,
    ) = more
    pieces = len(plan)
    send_y, recv_y, send_a, send_b, recv_a, recv_b = [
        rest[i * pieces : (i + 1) * pieces] for i in range(6)
    ]
    me = lax.axis_index("kv")
    col = lax.axis_index("tp")
    z, y = me // ny, lax.rem(me, ny)
    width = w_in.shape[1]
    sw = w_write.shape[1]
    local = tokens.shape[1]
    heads = bias.shape[1]
    seqs = own // DRAFT_TOKENS
    head_rows = own - own % 16
    tail_rows = own - head_rows
    block = nz * own
    full_rows = seqs * ROWS
    pad = tot_own.shape[0]
    groups = width // group_width
    per_group = group_width // P_SIZE

    step_cut = step_h.at[:, pl.ds(pl.multiple_of(me * local, 128), local)]
    pairs = [
        (tokens_h, tokens), (gain_h, gain), (step_cut, step_block), (write_h, w_write),
        (read_h, w_read), (in_h, w_in), (gate_h, w_gate), (bias_h, bias),
        (decay_h, decay), (extra_h, extra), (accepted_h, accepted),
        (saved_in_h, saved_in), (saved_write_h, saved_write), (saved_read_h, saved_read),
        (in_taps_h, in_taps), (write_taps_h, write_taps), (read_taps_h, read_taps),
        (bypass_h, bypass), (out_gain_h, out_gain), (matrix_h, matrix),
    ] + [(history_h.at[s], history.at[s]) for s in range(seqs)]
    last = (groups - 1) * group_width
    if groups > 1:
        pairs[6] = (gate_h.at[:, pl.ds(0, last)], w_gate.at[:, pl.ds(0, last)])
        pairs.append((
            gate_h.at[:, pl.ds(last, group_width)], w_gate.at[:, pl.ds(last, group_width)]
        ))
    loads = [
        pltpu.make_async_copy(source, target, load_sem.at[i])
        for i, (source, target) in enumerate(pairs)
    ]
    early = loads[20 + seqs] if groups > 1 else loads[6]
    for load in loads[:2] + [early] + [load for load in loads[2:11] if load is not early]:
        load.start()
    y_to = [{"kv": z * ny + lax.rem(y + d, ny)} for d in range(1, ny)]
    z_to = [{"kv": peer_to(z, d, nz) * ny + y} for d in range(1, nz)]
    cross = [
        [{"kv": peer_to(z, d, nz) * ny + lax.rem(y + e, ny)} for e in range(1, ny)]
        for d in range(1, nz)
    ]
    barrier = pltpu.get_barrier_semaphore()
    everyone = y_to + z_to + sum(cross, [])
    for peer in everyone:
        pl.semaphore_signal(barrier, inc=1, device_id=peer, device_id_type=MESH)
    for load in loads[11 : 20 + seqs]:
        load.start()

    loads[0].wait()
    loads[1].wait()
    wide[...] = tokens[...].astype(f32)
    for yy in range(ny):
        for zz in range(nz):
            source = (zz * ny + yy) * own
            at = zz * head_rows
            ordered[yy, at : at + head_rows] = wide[source : source + head_rows]
            if tail_rows:
                at = nz * head_rows + zz * tail_rows
                ordered[yy, at : at + tail_rows] = wide[source + head_rows : source + own]
    lane = iota((block, 128), 1)
    for yy in range(ny):
        values = ordered[yy]
        scaled[yy] = (values * gain[...]).astype(bf16)
        squares = jnp.sum(values * values, axis=1, keepdims=True)
        tail_squares[yy] = jnp.where(lane == heads, squares, 0.0)
    early.wait()
    for yy in range(ny):
        part = dot(scaled[yy], w_gate[:, last : last + group_width])
        for zz in range(nz):
            ez_send_a[zz, yy] = part[zz * head_rows : (zz + 1) * head_rows].astype(bf16)
            if tail_rows:
                at = nz * head_rows + zz * tail_rows
                ez_send_b[zz, yy] = part[at : at + tail_rows].astype(bf16)
    pl.semaphore_wait(barrier, len(everyone))
    ez_copies = []
    for d in reversed(range(1, nz)):
        to = peer_to(z, d, nz)
        for i, (buf, landing) in enumerate(((ez_send_a, ez_recv_a), (ez_send_b, ez_recv_b))):
            if i == 0 or tail_rows:
                copy = remote(
                    buf.at[to], landing.at[d - 1], ez_s.at[d - 1, i], ez_r.at[d - 1, i],
                    z_to[d - 1],
                )
                copy.start()
                ez_copies.append(copy)
    loads[2].wait()
    picked_row = iota((128, step_block.shape[0]), 0)
    pick = (iota((128, step_block.shape[0]), 1) == picked_row + col * heads) & (picked_row < heads)
    picked = dot(one_hot(pick), step_block[...]).astype(bf16)
    loads[3].wait()
    weights = {"read": w_read, "in": w_in, "gate": w_gate}

    def project(kind, first, size, at):
        rows = scaled[at]
        if kind == "write":
            return [
                (0, dot(rows, w_write[...])),
                (sw, tail_squares[at] + lax.dot_general(
                    rows, picked, (((1,), (1,)), ((), ())), preferred_element_type=f32
                )),
            ]
        return [(0, dot(rows, weights[kind][:, first : first + size]))]

    awaited = {}
    for kind, which in (("read", 4), ("in", 5), ("gate", 6)):
        for p in reversed(range(pieces)):
            if plan[p][0] == kind:
                awaited = {k: v for k, v in awaited.items() if k[0] != kind}
                awaited[kind, p] = loads[which]
    y_copies = []
    for p, (kind, first, size) in enumerate(plan):
        if (kind, p) in awaited:
            awaited[kind, p].wait()
        copies = []
        for d in range(1, ny):
            for at, part in project(kind, first, size, lax.rem(y + d, ny)):
                send_y[p][d - 1, :, at : at + part.shape[1]] = part.astype(bf16)
            copy = remote(
                send_y[p].at[d - 1], recv_y[p].at[d - 1], sy.at[p, d - 1], ry.at[p, d - 1],
                y_to[d - 1],
            )
            copy.start()
            copies.append(copy)
        y_copies.append(copies)

    offsets = []
    total_columns = 0
    for _, _, size in plan:
        offsets.append(total_columns)
        total_columns += size
    for p, (kind, first, size) in enumerate(plan):
        for at, part in project(kind, first, size, y):
            own_part[:, offsets[p] + at : offsets[p] + at + part.shape[1]] = part
    tot_own[...] = jnp.zeros_like(tot_own)
    y_all[...] = jnp.zeros_like(y_all)

    def early_total(buf, landing, at):
        total = buf[z, at].astype(f32)
        for d in range(1, nz):
            total = total + landing[d - 1, at].astype(f32)
        return total

    ey_copies = []

    def turn_early():
        for copy in ez_copies:
            copy.wait_recv()
        for d in range(1, ny):
            for i, (buf, landing, ready, arrived) in enumerate((
                (ez_send_a, ez_recv_a, ey_send_a, ey_recv_a),
                (ez_send_b, ez_recv_b, ey_send_b, ey_recv_b),
            )):
                if i == 0 or tail_rows:
                    ready[d - 1] = early_total(buf, landing, lax.rem(y + d, ny)).astype(bf16)
                    copy = remote(
                        ready.at[d - 1], arrived.at[d - 1], ey_s.at[d - 1, i],
                        ey_r.at[d - 1, i], y_to[d - 1],
                    )
                    copy.start()
                    ey_copies.append(copy)

    z_copies = []
    for p, (_, _, size) in enumerate(plan):
        if p == 3:
            turn_early()
        total = own_part[:, offsets[p] : offsets[p] + size]
        for d in range(1, ny):
            y_copies[p][d - 1].wait_recv()
            total = total + recv_y[p][d - 1].astype(f32)
        tot[:, :size] = total
        for zz in range(nz):
            at = zz * head_rows
            send_a[p][zz] = tot[at : at + head_rows, :size].astype(bf16)
            at = nz * head_rows + zz * tail_rows
            if tail_rows:
                send_b[p][zz] = tot[at : at + tail_rows, :size].astype(bf16)
        copies = []
        for d in reversed(range(1, nz)):
            to = peer_to(z, d, nz)
            for i, (buf, landing) in enumerate(((send_a, recv_a), (send_b, recv_b))):
                if i == 1 and not tail_rows:
                    continue
                copy = remote(
                    buf[p].at[to], landing[p].at[d - 1],
                    sz.at[p, d - 1, i], rz.at[p, d - 1, i], z_to[d - 1],
                )
                copy.start()
                copies.append(copy)
        z_copies.append(copies)

    if pieces <= 3:
        turn_early()
    row = iota((full_rows, pad), 0)
    column = iota((full_rows, pad), 1)
    seq_of, step_of = row // ROWS, lax.rem(row, ROWS)
    token = column - seq_of * DRAFT_TOKENS
    place_tok = one_hot((token == step_of) & (step_of < DRAFT_TOKENS))
    place_win = one_hot((token == step_of - LEAD) & (step_of >= LEAD))
    reach = ((token >= 0) & (token <= step_of) & (token < DRAFT_TOKENS)).astype(f32)
    square_row = iota((full_rows, full_rows), 0)
    square_column = iota((full_rows, full_rows), 1)
    for load in loads[7:19]:
        load.wait()
    taken = [accepted[s] for s in range(seqs)]
    shift = jnp.zeros((full_rows, full_rows), jnp.int32)
    for s in range(seqs):
        shift = jnp.where(square_row // ROWS == s, taken[s], shift)
    picks = one_hot(
        (square_column == square_row + shift) & (lax.rem(square_row, ROWS) < LEAD)
    )

    def gathered(p):
        size = plan[p][2]
        for copy in z_copies[p]:
            copy.wait_recv()
        total_a = send_a[p][z].astype(f32)
        for d in range(1, nz):
            total_a = total_a + recv_a[p][d - 1].astype(f32)
        tot_own[:head_rows, :size] = total_a
        if tail_rows:
            total_b = send_b[p][z].astype(f32)
            for d in range(1, nz):
                total_b = total_b + recv_b[p][d - 1].astype(f32)
            tot_own[head_rows:own, :size] = total_b
        return tot_own[:, :size]

    def gathered_early():
        for copy in ey_copies:
            copy.wait_recv()
        total = early_total(ez_send_a, ez_recv_a, y)
        for d in range(1, ny):
            total = total + ey_recv_a[d - 1].astype(f32)
        tot_own[:head_rows, :group_width] = total
        if tail_rows:
            total = early_total(ez_send_b, ez_recv_b, y)
            for d in range(1, ny):
                total = total + ey_recv_b[d - 1].astype(f32)
            tot_own[head_rows:own, :group_width] = total
        return tot_own[:, :group_width]

    def convolve(saved, fresh, taps, out):
        kept = saved.astype(f32).reshape(full_rows, saved.shape[2]).astype(bf16)
        window = dot(picks, kept) + dot(place_win, fresh)
        window = window.reshape(seqs, ROWS, saved.shape[2])
        out(window.astype(bf16))
        total = taps[0:1][None] * window
        for k in range(1, TAPS):
            total = total + taps[k : k + 1][None] * pltpu.roll(window, ROWS - k, 1)
        return jax.nn.silu(total).reshape(full_rows, saved.shape[2])

    def store(ref, cut):
        def put(value):
            ref[:, :, cut] = value
        return put

    small = gathered(0)
    tailing = small[:, sw:]
    inverse = lax.rsqrt(tailing[:, heads : heads + 1] / model_width + epsilon)
    steps = jax.nn.softplus(tailing[:, :heads] * inverse + bias[...])
    fresh = (small[:, :sw] * inverse).astype(bf16)
    w = convolve(saved_write[...], fresh, write_taps[...], store(next_write, slice(0, sw)))
    fresh = (gathered(1) * inverse).astype(bf16)
    r = convolve(saved_read[...], fresh, read_taps[...], store(next_read, slice(0, sw)))
    w_all[...] = w
    added_logs = lax.dot_general(
        (iota((pad, own), 0) == iota((pad, own), 1)).astype(f32), extra[...],
        (((1,), (1,)), ((), ())), precision=HIGH, preferred_element_type=f32,
    )
    logs = jnp.where(iota((pad, heads), 0) < own, -steps * jnp.exp(decay[...]) + added_logs, 0.0)
    summed = dot(reach, logs, precision=HIGH)
    steps_placed = dot(place_tok.astype(f32), steps, precision=HIGH)
    keep_all[...] = jnp.exp(summed)
    spread = (iota((heads, width), 0) == iota((heads, width), 1) // P_SIZE).astype(f32)
    stacked = jnp.concatenate(
        [summed, steps_placed, jnp.broadcast_to(bypass[...], (8, heads))], axis=0
    )
    spreaded = dot(stacked, spread, precision=HIGH)
    decay_all[...] = spreaded[:full_rows]
    step_all[...] = spreaded[full_rows : 2 * full_rows]
    direct = spreaded[2 * full_rows : 2 * full_rows + 1]
    mask_row = iota((ROWS, group_width), 0)
    for load in loads[20 : 20 + seqs]:
        load.wait()
    p_in = [p for p in range(pieces) if plan[p][0] == "in"]
    p_gate = [p for p in range(pieces) if plan[p][0] == "gate"]
    def push(g, chunk, sends, recvs, place):
        pair = []
        for i, buf in enumerate((all_a, all_b)):
            if i == 0 or tail_rows:
                pair.append(remote(
                    buf.at[g, chunk], buf.at[g, chunk], sends.at[i], recvs.at[i], place
                ))
                pair[-1].start()
        return pair

    straight = (0,)
    gz_copies = [[] for _ in range(groups)]
    gy_copies = [[] for _ in range(groups)]
    for p in p_in:
        g = plan[p][1] // group_width
        cut = slice(g * group_width, (g + 1) * group_width)
        fresh = (gathered(p) * inverse).astype(bf16)
        x = convolve(saved_in[:, :, cut], fresh, in_taps[:, cut], store(next_in, cut))
        step_x = step_all[:, cut] * x
        step_all[:, cut] = step_x
        through = direct[:, cut] * x
        for s in range(seqs):
            rs = slice(s * ROWS, (s + 1) * ROWS)
            wg, rg = w[rs, g * N : (g + 1) * N], r[rs, g * N : (g + 1) * N]
            start = history[s, taken[s], g * per_group : (g + 1) * per_group].reshape(group_width, N)
            out = lax.dot_general(
                rg.astype(bf16), start.astype(bf16), (((1,), (1,)), ((), ())),
                preferred_element_type=f32,
            )
            dg, sg = decay_all[rs, cut], step_x[rs]
            out = out * jnp.exp(dg) + through[rs]
            overlap = lax.dot_general(
                rg, wg, (((1,), (1,)), ((), ())), precision=HIGH, preferred_element_type=f32
            )
            for j in range(DRAFT_TOKENS):
                live = mask_row >= j
                fade = jnp.exp(jnp.where(live, dg - dg[j : j + 1], 0.0))
                out = out + jnp.where(live, fade * overlap[:, j : j + 1] * sg[j : j + 1], 0.0)
            y_all[s * DRAFT_TOKENS : (s + 1) * DRAFT_TOKENS, cut] = out[:DRAFT_TOKENS]

        parts = []
        if g == groups - 1:
            parts.append((gathered_early() * inverse).astype(bf16).astype(f32))
        for p_of in p_gate:
            if cut.start <= plan[p_of][1] < cut.stop:
                parts.append((gathered(p_of) * inverse).astype(bf16).astype(f32))
        gate = parts[0] if len(parts) == 1 else jnp.concatenate(parts, axis=1)
        gated = y_all[:, cut] * (gate * jax.nn.sigmoid(gate))
        gated = gated * lax.rsqrt(jnp.mean(gated * gated, axis=1, keepdims=True) + epsilon)
        normed = (gated * out_gain[:, cut]).astype(bf16)
        all_a[g, me] = normed[:head_rows]
        if tail_rows:
            all_b[g, me] = normed[head_rows:own]
        for d in reversed(range(1, nz)):
            gz_copies[g].insert(
                0, push(g, me, gz_s.at[g, d - 1], gz_r.at[g, d - 1], z_to[d - 1])
            )
            if g in straight:
                gy_copies[g] += [
                    push(g, me, gy_s.at[g, d, e], gy_r.at[g, d, e], cross[d - 1][e])
                    for e in range(ny - 1)
                ]
        gy_copies[g] += [
            push(g, me, gy_s.at[g, 0, e], gy_r.at[g, 0, e], y_to[e]) for e in range(ny - 1)
        ]

    for s in range(seqs):
        rs = slice(s * ROWS, (s + 1) * ROWS)
        keep = keep_all[rs]
        for g in range(groups):
            cut = slice(g * group_width, (g + 1) * group_width)
            wg, dg, sg = w_all[rs, g * N : (g + 1) * N], decay_all[rs, cut], step_all[rs, cut]
            terms = []
            sides = []
            wide_w = jnp.concatenate([wg] * DRAFT_TOKENS, axis=1)
            wide_lane = iota(wide_w.shape, 1) // N
            for t in range(DRAFT_TOKENS):
                live = mask_row <= t
                fade = jnp.exp(jnp.where(live, dg[t : t + 1] - dg, 0.0))
                terms.append(jnp.where(live, fade * sg, 0.0))
                sides.append(jnp.where(wide_lane == t, wide_w, 0.0))
            left = jnp.concatenate(terms, axis=0).T.astype(bf16)
            added = dot(left, jnp.concatenate(sides, axis=0).astype(bf16))
            for i in range(per_group):
                h = g * per_group + i
                held = history[s, taken[s], h]
                states[s, 0, h] = held
                for t in range(DRAFT_TOKENS):
                    factor_th = jnp.broadcast_to(keep[t : t + 1, h : h + 1], (P_SIZE, N))
                    states[s, t + 1, h] = (
                        factor_th * held
                        + added[i * P_SIZE : (i + 1) * P_SIZE, t * N : (t + 1) * N]
                    )

    for g in reversed(range(groups)):
        for d in range(1, nz):
            for copy in gz_copies[g][d - 1]:
                copy.wait_recv()
            if g not in straight:
                chunk = peer_from(z, d, nz) * ny + y
                gy_copies[g] += [
                    push(g, chunk, gy_s.at[g, d, e], gy_r.at[g, d, e], y_to[e])
                    for e in range(ny - 1)
                ]
    loads[19].wait()
    for g in range(groups):
        for pair in gy_copies[g]:
            for copy in pair:
                copy.wait_recv()
        for k in range(nz * ny):
            if tail_rows:
                rows_b[g, k * tail_rows : (k + 1) * tail_rows] = all_b[g, k].astype(f32)
    each = nz * ny // nt

    span = nz * ny * head_rows
    product = 0.0
    for g in range(groups):
        left = all_a[g].reshape(span, group_width)
        if tail_rows:
            left = jnp.concatenate([left, rows_b[g].astype(bf16)], axis=0)
        product = product + dot(left, matrix[g * group_width : (g + 1) * group_width])
    for t in range(nt):
        for k in range(each):
            at = (t * each + k) * head_rows
            final[t, k * own : k * own + head_rows] = product[at : at + head_rows]
            if tail_rows:
                at = span + (t * each + k) * tail_rows
                final[t, k * own + head_rows : (k + 1) * own] = product[at : at + tail_rows]
    for d in reversed(range(1, nt)):
        away[d - 1][...] = final[peer_to(col, d, nt)].astype(bf16)
    mix[...] = final[col]
    for copies in y_copies + z_copies + [ez_copies, ey_copies]:
        for copy in copies:
            copy.wait_send()
    for pairs_of in gz_copies + gy_copies:
        for pair in pairs_of:
            for copy in pair:
                copy.wait_send()


def emit_kernel(
    states, next_in, next_write, next_read,
    states_h, next_in_h, next_write_h, next_read_h, sem,
):
    pairs = [
        (states.at[s, t], states_h.at[s, t])
        for s in range(states.shape[0]) for t in range(states.shape[1])
    ] + [
        (next_in, next_in_h), (next_write, next_write_h), (next_read, next_read_h),
    ]
    copies = [
        pltpu.make_async_copy(source, target, sem.at[i])
        for i, (source, target) in enumerate(pairs)
    ]
    for copy in copies:
        copy.start()
    for copy in copies:
        copy.wait()


def per_device(
    tokens, input_norm_gain, input_matrix, gate_matrix, write_matrix, read_matrix, step_matrix,
    input_kernel, write_kernel, read_kernel, step_size_bias, head_decay_logs, bypass_scale,
    extra_decay_logs, output_norm_gain, output_matrix, cached_state_history,
    cached_input_rows, cached_write_rows, cached_read_rows, accepted,
):
    kv = lax.axis_size("kv")
    nt = lax.axis_size("tp")
    nz, ny = factor(kv)
    own = tokens.shape[0] // kv
    head_rows = own - own % 16
    tail_rows = max(own - head_rows, 1)
    seqs = own // DRAFT_TOKENS
    full_rows = seqs * ROWS
    pad = -(-own // 16) * 16
    block = nz * own
    local = tokens.shape[1]
    heads = step_size_bias.shape[0]
    width = input_matrix.shape[1]
    sw = write_matrix.shape[1]
    group_width = width // (sw // N)
    groups = width // group_width
    half = group_width // 2
    out_width = output_matrix.shape[1]
    each = kv // nt
    vmem = pl.BlockSpec(memory_space=pltpu.VMEM)
    hbm = pl.BlockSpec(memory_space=pltpu.HBM)
    plan = [("write", 0, sw + 128), ("read", 0, sw)]
    plan += [("in", g * group_width, group_width) for g in reversed(range(groups))]
    plan += [("gate", g * group_width, group_width) for g in reversed(range(1, groups - 1))]
    if groups > 1:
        plan += [("gate", 0, half), ("gate", half, half)]
    sizes = [size for _, _, size in plan]
    pieces = len(plan)
    dma = pltpu.SemaphoreType.DMA
    peers = max(ny - 1, 1)
    shape = jax.ShapeDtypeStruct
    operands = (
        tokens, input_norm_gain[None], input_matrix, gate_matrix, write_matrix, read_matrix,
        step_matrix.T, step_size_bias[None], head_decay_logs[None], extra_decay_logs.T,
        input_kernel, write_kernel, read_kernel, bypass_scale[None], output_norm_gain[None],
        output_matrix, cached_state_history, cached_input_rows, cached_write_rows,
        cached_read_rows, accepted,
    )
    step_shape = (step_matrix.shape[1], local)
    buffers = [
        pltpu.VMEM(step_shape if i == 6 else a.shape, a.dtype)
        for i, a in enumerate(operands[:-1])
    ]
    part = (each * own, out_width)
    results = (
        (cached_state_history.shape, f32), (cached_input_rows.shape, bf16),
        (cached_write_rows.shape, bf16), (cached_read_rows.shape, bf16),
    )
    everything = ((part, f32),) + ((part, bf16),) * (nt - 1) + results
    outs = pl.pallas_call(
        functools.partial(
            mixer_kernel, nz, ny, nt, own, local * kv, tuple(plan), group_width
        ),
        out_shape=tuple(pltpu.VMEM(dims, kind) for dims, kind in everything),
        in_specs=[hbm] * len(operands),
        out_specs=[vmem] * len(everything),
        scratch_shapes=buffers + [
            pltpu.SMEM(accepted.shape, jnp.int32),
            dma((len(operands) + seqs,)),
            pltpu.VMEM(tokens.shape, f32),
            pltpu.VMEM((ny, block, local), f32),
            pltpu.VMEM((ny, block, local), bf16),
            pltpu.VMEM((ny, block, 128), f32),
            pltpu.VMEM((block, sum(sizes)), f32),
            pltpu.VMEM((block, max(sizes)), f32),
            pltpu.VMEM((pad, max(sizes)), f32),
            pltpu.VMEM((pad, width), f32),
            pltpu.VMEM((full_rows, heads), f32),
            pltpu.VMEM((full_rows, width), f32),
            pltpu.VMEM((full_rows, width), f32),
            pltpu.VMEM((full_rows, sw), f32),
            pltpu.VMEM((groups, kv, head_rows, group_width), bf16),
            pltpu.VMEM((groups, kv, tail_rows, group_width), bf16),
            pltpu.VMEM((groups, kv * tail_rows, group_width), f32),
            pltpu.VMEM((nt, each * own, out_width), f32),
            dma((pieces, peers)), dma((pieces, peers)),
            dma((pieces, nz - 1, 2)), dma((pieces, nz - 1, 2)),
            dma((groups, nz - 1, 2)), dma((groups, nz - 1, 2)),
            dma((groups, nz, peers, 2)), dma((groups, nz, peers, 2)),
            pltpu.VMEM((nz, ny, head_rows, group_width), bf16),
            pltpu.VMEM((nz, ny, tail_rows, group_width), bf16),
            pltpu.VMEM((nz - 1, ny, head_rows, group_width), bf16),
            pltpu.VMEM((nz - 1, ny, tail_rows, group_width), bf16),
            pltpu.VMEM((peers, head_rows, group_width), bf16),
            pltpu.VMEM((peers, tail_rows, group_width), bf16),
            pltpu.VMEM((peers, head_rows, group_width), bf16),
            pltpu.VMEM((peers, tail_rows, group_width), bf16),
            dma((nz - 1, 2)), dma((nz - 1, 2)), dma((peers, 2)), dma((peers, 2)),
        ]
        + [pltpu.VMEM((peers, block, c), bf16) for c in sizes]
        + [pltpu.VMEM((peers, block, c), bf16) for c in sizes]
        + [pltpu.VMEM((nz, head_rows, c), bf16) for c in sizes]
        + [pltpu.VMEM((nz, tail_rows, c), bf16) for c in sizes]
        + [pltpu.VMEM((nz - 1, head_rows, c), bf16) for c in sizes]
        + [pltpu.VMEM((nz - 1, tail_rows, c), bf16) for c in sizes],
        compiler_params=pltpu.CompilerParams(
            collective_id=0, has_side_effects=True, vmem_limit_bytes=40 * 2**20
        ),
    )(*[pltpu.with_memory_space_constraint(a, pltpu.HBM) for a in operands])
    kept = pl.pallas_call(
        emit_kernel,
        out_shape=tuple(shape(dims, kind) for dims, kind in results),
        in_specs=[vmem] * len(results),
        out_specs=[hbm] * len(results),
        scratch_shapes=[dma((seqs * (DRAFT_TOKENS + 1) + len(results) - 1,))],
        compiler_params=pltpu.CompilerParams(vmem_limit_bytes=2**20),
        cost_estimate=pl.CostEstimate(flops=10**8, bytes_accessed=10**7, transcendentals=0),
    )(*outs[nt:])
    total = outs[0]
    for d in range(1, nt):
        ring = [(i, static_to(i, d, nt)) for i in range(nt)]
        total = total + lax.ppermute(outs[d], "tp", ring).astype(f32)
    return (total.astype(bf16),) + tuple(kept)


def solution(mesh):
    return jax.shard_map(
        per_device,
        mesh=mesh,
        in_specs=(
            P(None, "kv"),
            P("kv"),
            P("kv", "tp"),
            P("kv", "tp"),
            P("kv", "tp"),
            P("kv", "tp"),
            P(),
            P(None, "tp"),
            P(None, "tp"),
            P(None, "tp"),
            P("tp"),
            P("tp"),
            P("tp"),
            P("kv", "tp"),
            P("tp"),
            P("tp", "kv"),
            P("kv", None, "tp", None, None),
            P("kv", None, "tp"),
            P("kv", None, "tp"),
            P("kv", None, "tp"),
            P("kv"),
        ),
        out_specs=(
            P("tp", "kv"),
            P("kv", None, "tp", None, None),
            P("kv", None, "tp"),
            P("kv", None, "tp"),
            P("kv", None, "tp"),
        ),
        check_vma=False,
    )
```

```python
import functools

import jax
import jax.numpy as jnp
from jax import lax
from jax.experimental import pallas as pl
from jax.experimental.pallas import tpu as pltpu
from jax.sharding import PartitionSpec as P

P_SIZE = 64
N = 128
TAPS = 4
DRAFT_TOKENS = 5
ROWS = DRAFT_TOKENS + TAPS - 1
LEAD = TAPS - 1
MESH = pl.DeviceIdType.MESH
HIGH = lax.Precision.HIGHEST
f32, bf16 = jnp.float32, jnp.bfloat16
epsilon = 1e-05


def factor(count):
    low = max(d for d in range(1, count + 1) if count % d == 0 and d * d <= count)
    return count // low, low


def paired(count):
    return count in (1, 2, 4)


def peer_to(me, d, count):
    if d == 0:
        return me
    if not paired(count):
        return lax.rem(me + d, count)
    if d == count // 2:
        return lax.rem(me + d, count)
    if d == count - 1:
        return count - 1 - me
    return me + 1 - 2 * lax.rem(me, 2)


def static_to(me, d, count):
    return me ^ d if paired(count) else (me + d) % count


def peer_from(me, d, count):
    if not paired(count):
        return lax.rem(me - d + count, count)
    return peer_to(me, d, count)


def remote(src, dst, send, recv, where):
    return pltpu.make_async_remote_copy(
        src_ref=src, dst_ref=dst, send_sem=send, recv_sem=recv, device_id=where, device_id_type=MESH
    )


def iota(shape, dim):
    return lax.broadcasted_iota(jnp.int32, shape, dim)


def one_hot(mask):
    return mask.astype(f32).astype(bf16)


def dot(a, b, **more):
    return jnp.dot(a, b, preferred_element_type=f32, **more)


def mixer_kernel(
    nz, ny, nt, own, model_width, plan, group_width,
    tokens_h, gain_h, in_h, gate_h, write_h, read_h, step_h, bias_h, decay_h, extra_h,
    in_taps_h, write_taps_h, read_taps_h, bypass_h, out_gain_h, matrix_h,
    history_h, saved_in_h, saved_write_h, saved_read_h, accepted_h,
    mix, *more,
):
    away, more = more[: nt - 1], more[nt - 1 :]
    (states, next_in, next_write, next_read), more = more[:4], more[4:]
    (
    tokens, gain, w_in, w_gate, w_write, w_read, step_block, bias, decay, extra,
    in_taps, write_taps, read_taps, bypass, out_gain, matrix,
    history, saved_in, saved_write, saved_read, accepted, load_sem,
    wide, ordered, scaled, tail_squares, own_part, tot, tot_own, y_all, keep_all, decay_all,
    step_all, w_all,
    all_a, all_b, rows_b, final,
    sy, ry, sz, rz, gz_s, gz_r, gy_s, gy_r,
    ez_send_a, ez_send_b, ez_recv_a, ez_recv_b, ey_send_a, ey_send_b, ey_recv_a, ey_recv_b,
    ez_s, ez_r, ey_s, ey_r, *rest,
    ) = more
    pieces = len(plan)
    send_y, recv_y, send_a, send_b, recv_a, recv_b = [
        rest[i * pieces : (i + 1) * pieces] for i in range(6)
    ]
    me = lax.axis_index("kv")
    col = lax.axis_index("tp")
    z, y = me // ny, lax.rem(me, ny)
    width = w_in.shape[1]
    sw = w_write.shape[1]
    local = tokens.shape[1]
    heads = bias.shape[1]
    seqs = own // DRAFT_TOKENS
    head_rows = own - own % 16
    tail_rows = own - head_rows
    block = nz * own
    full_rows = seqs * ROWS
    pad = tot_own.shape[0]
    groups = width // group_width
    per_group = group_width // P_SIZE

    step_cut = step_h.at[:, pl.ds(pl.multiple_of(me * local, 128), local)]
    pairs = [
        (tokens_h, tokens), (gain_h, gain), (step_cut, step_block), (write_h, w_write),
        (read_h, w_read), (in_h, w_in), (gate_h, w_gate), (bias_h, bias),
        (decay_h, decay), (extra_h, extra), (accepted_h, accepted),
        (saved_in_h, saved_in), (saved_write_h, saved_write), (saved_read_h, saved_read),
        (in_taps_h, in_taps), (write_taps_h, write_taps), (read_taps_h, read_taps),
        (bypass_h, bypass), (out_gain_h, out_gain), (matrix_h, matrix),
    ] + [(history_h.at[s], history.at[s]) for s in range(seqs)]
    last = (groups - 1) * group_width
    if groups > 1:
        pairs[6] = (gate_h.at[:, pl.ds(0, last)], w_gate.at[:, pl.ds(0, last)])
        pairs.append((
            gate_h.at[:, pl.ds(last, group_width)], w_gate.at[:, pl.ds(last, group_width)]
        ))
    loads = [
        pltpu.make_async_copy(source, target, load_sem.at[i])
        for i, (source, target) in enumerate(pairs)
    ]
    early = loads[20 + seqs] if groups > 1 else loads[6]
    for load in loads[:4] + [early] + [load for load in loads[4:11] if load is not early]:
        load.start()
    y_to = [{"kv": z * ny + lax.rem(y + d, ny)} for d in range(1, ny)]
    z_to = [{"kv": peer_to(z, d, nz) * ny + y} for d in range(1, nz)]
    cross = [
        [{"kv": peer_to(z, d, nz) * ny + lax.rem(y + e, ny)} for e in range(1, ny)]
        for d in range(1, nz)
    ]
    barrier = pltpu.get_barrier_semaphore()
    everyone = y_to + z_to + sum(cross, [])
    for peer in everyone:
        pl.semaphore_signal(barrier, inc=1, device_id=peer, device_id_type=MESH)
    for load in loads[11 : 20 + seqs]:
        load.start()

    loads[0].wait()
    loads[1].wait()
    wide[...] = tokens[...].astype(f32)
    for yy in range(ny):
        for zz in range(nz):
            source = (zz * ny + yy) * own
            at = zz * head_rows
            ordered[yy, at : at + head_rows] = wide[source : source + head_rows]
            if tail_rows:
                at = nz * head_rows + zz * tail_rows
                ordered[yy, at : at + tail_rows] = wide[source + head_rows : source + own]
    lane = iota((block, 128), 1)
    for yy in range(ny):
        values = ordered[yy]
        scaled[yy] = (values * gain[...]).astype(bf16)
        squares = jnp.sum(values * values, axis=1, keepdims=True)
        tail_squares[yy] = jnp.where(lane == heads, squares, 0.0)
    loads[2].wait()
    picked_row = iota((128, step_block.shape[0]), 0)
    pick = (iota((128, step_block.shape[0]), 1) == picked_row + col * heads) & (picked_row < heads)
    picked = dot(one_hot(pick), step_block[...]).astype(bf16)
    loads[3].wait()
    weights = {"read": w_read, "in": w_in, "gate": w_gate}

    def project(kind, first, size, at):
        rows = scaled[at]
        if kind == "write":
            return [
                (0, dot(rows, w_write[...])),
                (sw, tail_squares[at] + lax.dot_general(
                    rows, picked, (((1,), (1,)), ((), ())), preferred_element_type=f32
                )),
            ]
        return [(0, dot(rows, weights[kind][:, first : first + size]))]

    awaited = {}
    for kind, which in (("read", 4), ("in", 5), ("gate", 6)):
        for p in reversed(range(pieces)):
            if plan[p][0] == kind:
                awaited = {k: v for k, v in awaited.items() if k[0] != kind}
                awaited[kind, p] = loads[which]
    ez_copies = []

    def send_early():
        early.wait()
        for yy in range(ny):
            part = dot(scaled[yy], w_gate[:, last : last + group_width])
            for zz in range(nz):
                ez_send_a[zz, yy] = part[zz * head_rows : (zz + 1) * head_rows].astype(bf16)
                if tail_rows:
                    at = nz * head_rows + zz * tail_rows
                    ez_send_b[zz, yy] = part[at : at + tail_rows].astype(bf16)
        for d in reversed(range(1, nz)):
            to = peer_to(z, d, nz)
            for i, (buf, landing) in enumerate(((ez_send_a, ez_recv_a), (ez_send_b, ez_recv_b))):
                if i == 0 or tail_rows:
                    copy = remote(
                        buf.at[to], landing.at[d - 1], ez_s.at[d - 1, i], ez_r.at[d - 1, i],
                        z_to[d - 1],
                    )
                    copy.start()
                    ez_copies.append(copy)

    y_copies = []
    if ny == 1:
        pl.semaphore_wait(barrier, len(everyone))
    for p, (kind, first, size) in enumerate(plan):
        if (kind, p) in awaited:
            awaited[kind, p].wait()
        copies = []
        for d in range(1, ny):
            for at, part in project(kind, first, size, lax.rem(y + d, ny)):
                send_y[p][d - 1, :, at : at + part.shape[1]] = part.astype(bf16)
            if p == 0 and d == 1:
                pl.semaphore_wait(barrier, len(everyone))
            copy = remote(
                send_y[p].at[d - 1], recv_y[p].at[d - 1], sy.at[p, d - 1], ry.at[p, d - 1],
                y_to[d - 1],
            )
            copy.start()
            copies.append(copy)
        y_copies.append(copies)
        if p == 0:
            send_early()

    offsets = []
    total_columns = 0
    for _, _, size in plan:
        offsets.append(total_columns)
        total_columns += size
    for p, (kind, first, size) in enumerate(plan):
        for at, part in project(kind, first, size, y):
            own_part[:, offsets[p] + at : offsets[p] + at + part.shape[1]] = part
    tot_own[...] = jnp.zeros_like(tot_own)
    y_all[...] = jnp.zeros_like(y_all)

    def early_total(buf, landing, at):
        total = buf[z, at].astype(f32)
        for d in range(1, nz):
            total = total + landing[d - 1, at].astype(f32)
        return total

    ey_copies = []

    def turn_early():
        for copy in ez_copies:
            copy.wait_recv()
        for d in range(1, ny):
            for i, (buf, landing, ready, arrived) in enumerate((
                (ez_send_a, ez_recv_a, ey_send_a, ey_recv_a),
                (ez_send_b, ez_recv_b, ey_send_b, ey_recv_b),
            )):
                if i == 0 or tail_rows:
                    ready[d - 1] = early_total(buf, landing, lax.rem(y + d, ny)).astype(bf16)
                    copy = remote(
                        ready.at[d - 1], arrived.at[d - 1], ey_s.at[d - 1, i],
                        ey_r.at[d - 1, i], y_to[d - 1],
                    )
                    copy.start()
                    ey_copies.append(copy)

    z_copies = []
    for p, (_, _, size) in enumerate(plan):
        if p == 3:
            turn_early()
        total = own_part[:, offsets[p] : offsets[p] + size]
        for d in range(1, ny):
            y_copies[p][d - 1].wait_recv()
            total = total + recv_y[p][d - 1].astype(f32)
        tot[:, :size] = total
        for zz in range(nz):
            at = zz * head_rows
            send_a[p][zz] = tot[at : at + head_rows, :size].astype(bf16)
            at = nz * head_rows + zz * tail_rows
            if tail_rows:
                send_b[p][zz] = tot[at : at + tail_rows, :size].astype(bf16)
        copies = []
        for d in reversed(range(1, nz)):
            to = peer_to(z, d, nz)
            for i, (buf, landing) in enumerate(((send_a, recv_a), (send_b, recv_b))):
                if i == 1 and not tail_rows:
                    continue
                copy = remote(
                    buf[p].at[to], landing[p].at[d - 1],
                    sz.at[p, d - 1, i], rz.at[p, d - 1, i], z_to[d - 1],
                )
                copy.start()
                copies.append(copy)
        z_copies.append(copies)

    if pieces <= 3:
        turn_early()
    row = iota((full_rows, pad), 0)
    column = iota((full_rows, pad), 1)
    seq_of, step_of = row // ROWS, lax.rem(row, ROWS)
    token = column - seq_of * DRAFT_TOKENS
    place_tok = one_hot((token == step_of) & (step_of < DRAFT_TOKENS))
    place_win = one_hot((token == step_of - LEAD) & (step_of >= LEAD))
    reach = ((token >= 0) & (token <= step_of) & (token < DRAFT_TOKENS)).astype(f32)
    square_row = iota((full_rows, full_rows), 0)
    square_column = iota((full_rows, full_rows), 1)
    for load in loads[7:19]:
        load.wait()
    taken = [accepted[s] for s in range(seqs)]
    shift = jnp.zeros((full_rows, full_rows), jnp.int32)
    for s in range(seqs):
        shift = jnp.where(square_row // ROWS == s, taken[s], shift)
    picks = one_hot(
        (square_column == square_row + shift) & (lax.rem(square_row, ROWS) < LEAD)
    )

    def gathered(p):
        size = plan[p][2]
        for copy in z_copies[p]:
            copy.wait_recv()
        total_a = send_a[p][z].astype(f32)
        for d in range(1, nz):
            total_a = total_a + recv_a[p][d - 1].astype(f32)
        tot_own[:head_rows, :size] = total_a
        if tail_rows:
            total_b = send_b[p][z].astype(f32)
            for d in range(1, nz):
                total_b = total_b + recv_b[p][d - 1].astype(f32)
            tot_own[head_rows:own, :size] = total_b
        return tot_own[:, :size]

    def gathered_early():
        for copy in ey_copies:
            copy.wait_recv()
        total = early_total(ez_send_a, ez_recv_a, y)
        for d in range(1, ny):
            total = total + ey_recv_a[d - 1].astype(f32)
        tot_own[:head_rows, :group_width] = total
        if tail_rows:
            total = early_total(ez_send_b, ez_recv_b, y)
            for d in range(1, ny):
                total = total + ey_recv_b[d - 1].astype(f32)
            tot_own[head_rows:own, :group_width] = total
        return tot_own[:, :group_width]

    def convolve(saved, fresh, taps, out):
        kept = saved.astype(f32).reshape(full_rows, saved.shape[2]).astype(bf16)
        window = dot(picks, kept) + dot(place_win, fresh)
        window = window.reshape(seqs, ROWS, saved.shape[2])
        out(window.astype(bf16))
        total = taps[0:1][None] * window
        for k in range(1, TAPS):
            total = total + taps[k : k + 1][None] * pltpu.roll(window, ROWS - k, 1)
        return jax.nn.silu(total).reshape(full_rows, saved.shape[2])

    def store(ref, cut):
        def put(value):
            ref[:, :, cut] = value
        return put

    small = gathered(0)
    tailing = small[:, sw:]
    inverse = lax.rsqrt(tailing[:, heads : heads + 1] / model_width + epsilon)
    steps = jax.nn.softplus(tailing[:, :heads] * inverse + bias[...])
    fresh = (small[:, :sw] * inverse).astype(bf16)
    w = convolve(saved_write[...], fresh, write_taps[...], store(next_write, slice(0, sw)))
    fresh = (gathered(1) * inverse).astype(bf16)
    r = convolve(saved_read[...], fresh, read_taps[...], store(next_read, slice(0, sw)))
    w_all[...] = w
    added_logs = lax.dot_general(
        (iota((pad, own), 0) == iota((pad, own), 1)).astype(f32), extra[...],
        (((1,), (1,)), ((), ())), precision=HIGH, preferred_element_type=f32,
    )
    logs = jnp.where(iota((pad, heads), 0) < own, -steps * jnp.exp(decay[...]) + added_logs, 0.0)
    summed = dot(reach, logs, precision=HIGH)
    steps_placed = dot(place_tok.astype(f32), steps, precision=HIGH)
    keep_all[...] = jnp.exp(summed)
    spread = (iota((heads, width), 0) == iota((heads, width), 1) // P_SIZE).astype(f32)
    stacked = jnp.concatenate(
        [summed, steps_placed, jnp.broadcast_to(bypass[...], (8, heads))], axis=0
    )
    spreaded = dot(stacked, spread, precision=HIGH)
    decay_all[...] = spreaded[:full_rows]
    step_all[...] = spreaded[full_rows : 2 * full_rows]
    direct = spreaded[2 * full_rows : 2 * full_rows + 1]
    mask_row = iota((ROWS, group_width), 0)
    for load in loads[20 : 20 + seqs]:
        load.wait()
    p_in = [p for p in range(pieces) if plan[p][0] == "in"]
    p_gate = [p for p in range(pieces) if plan[p][0] == "gate"]
    def push(g, chunk, sends, recvs, place):
        pair = []
        for i, buf in enumerate((all_a, all_b)):
            if i == 0 or tail_rows:
                pair.append(remote(
                    buf.at[g, chunk], buf.at[g, chunk], sends.at[i], recvs.at[i], place
                ))
                pair[-1].start()
        return pair

    straight = (0,)
    gz_copies = [[] for _ in range(groups)]
    gy_copies = [[] for _ in range(groups)]
    for p in p_in:
        g = plan[p][1] // group_width
        cut = slice(g * group_width, (g + 1) * group_width)
        fresh = (gathered(p) * inverse).astype(bf16)
        x = convolve(saved_in[:, :, cut], fresh, in_taps[:, cut], store(next_in, cut))
        step_x = step_all[:, cut] * x
        step_all[:, cut] = step_x
        through = direct[:, cut] * x
        for s in range(seqs):
            rs = slice(s * ROWS, (s + 1) * ROWS)
            wg, rg = w[rs, g * N : (g + 1) * N], r[rs, g * N : (g + 1) * N]
            start = history[s, taken[s], g * per_group : (g + 1) * per_group].reshape(group_width, N)
            out = lax.dot_general(
                rg.astype(bf16), start.astype(bf16), (((1,), (1,)), ((), ())),
                preferred_element_type=f32,
            )
            dg, sg = decay_all[rs, cut], step_x[rs]
            out = out * jnp.exp(dg) + through[rs]
            overlap = lax.dot_general(
                rg, wg, (((1,), (1,)), ((), ())), precision=HIGH, preferred_element_type=f32
            )
            for j in range(DRAFT_TOKENS):
                live = mask_row >= j
                fade = jnp.exp(jnp.where(live, dg - dg[j : j + 1], 0.0))
                out = out + jnp.where(live, fade * overlap[:, j : j + 1] * sg[j : j + 1], 0.0)
            y_all[s * DRAFT_TOKENS : (s + 1) * DRAFT_TOKENS, cut] = out[:DRAFT_TOKENS]

        parts = []
        if g == groups - 1:
            parts.append((gathered_early() * inverse).astype(bf16).astype(f32))
        for p_of in p_gate:
            if cut.start <= plan[p_of][1] < cut.stop:
                parts.append((gathered(p_of) * inverse).astype(bf16).astype(f32))
        gate = parts[0] if len(parts) == 1 else jnp.concatenate(parts, axis=1)
        gated = y_all[:, cut] * (gate * jax.nn.sigmoid(gate))
        gated = gated * lax.rsqrt(jnp.mean(gated * gated, axis=1, keepdims=True) + epsilon)
        normed = (gated * out_gain[:, cut]).astype(bf16)
        all_a[g, me] = normed[:head_rows]
        if tail_rows:
            all_b[g, me] = normed[head_rows:own]
        for d in reversed(range(1, nz)):
            gz_copies[g].insert(
                0, push(g, me, gz_s.at[g, d - 1], gz_r.at[g, d - 1], z_to[d - 1])
            )
            if g in straight:
                gy_copies[g] += [
                    push(g, me, gy_s.at[g, d, e], gy_r.at[g, d, e], cross[d - 1][e])
                    for e in range(ny - 1)
                ]
        gy_copies[g] += [
            push(g, me, gy_s.at[g, 0, e], gy_r.at[g, 0, e], y_to[e]) for e in range(ny - 1)
        ]

    for s in range(seqs):
        rs = slice(s * ROWS, (s + 1) * ROWS)
        keep = keep_all[rs]
        for g in range(groups):
            cut = slice(g * group_width, (g + 1) * group_width)
            wg, dg, sg = w_all[rs, g * N : (g + 1) * N], decay_all[rs, cut], step_all[rs, cut]
            terms = []
            sides = []
            wide_w = jnp.concatenate([wg] * DRAFT_TOKENS, axis=1)
            wide_lane = iota(wide_w.shape, 1) // N
            for t in range(DRAFT_TOKENS):
                live = mask_row <= t
                fade = jnp.exp(jnp.where(live, dg[t : t + 1] - dg, 0.0))
                terms.append(jnp.where(live, fade * sg, 0.0))
                sides.append(jnp.where(wide_lane == t, wide_w, 0.0))
            left = jnp.concatenate(terms, axis=0).T.astype(bf16)
            added = dot(left, jnp.concatenate(sides, axis=0).astype(bf16))
            for i in range(per_group):
                h = g * per_group + i
                held = history[s, taken[s], h]
                states[s, 0, h] = held
                for t in range(DRAFT_TOKENS):
                    factor_th = jnp.broadcast_to(keep[t : t + 1, h : h + 1], (P_SIZE, N))
                    states[s, t + 1, h] = (
                        factor_th * held
                        + added[i * P_SIZE : (i + 1) * P_SIZE, t * N : (t + 1) * N]
                    )

    for g in reversed(range(groups)):
        for d in range(1, nz):
            for copy in gz_copies[g][d - 1]:
                copy.wait_recv()
            if g not in straight:
                chunk = peer_from(z, d, nz) * ny + y
                gy_copies[g] += [
                    push(g, chunk, gy_s.at[g, d, e], gy_r.at[g, d, e], y_to[e])
                    for e in range(ny - 1)
                ]
    loads[19].wait()
    for g in range(groups):
        for pair in gy_copies[g]:
            for copy in pair:
                copy.wait_recv()
        for k in range(nz * ny):
            if tail_rows:
                rows_b[g, k * tail_rows : (k + 1) * tail_rows] = all_b[g, k].astype(f32)
    each = nz * ny // nt

    span = nz * ny * head_rows
    product = 0.0
    for g in range(groups):
        left = all_a[g].reshape(span, group_width)
        if tail_rows:
            left = jnp.concatenate([left, rows_b[g].astype(bf16)], axis=0)
        product = product + dot(left, matrix[g * group_width : (g + 1) * group_width])
    for t in range(nt):
        for k in range(each):
            at = (t * each + k) * head_rows
            final[t, k * own : k * own + head_rows] = product[at : at + head_rows]
            if tail_rows:
                at = span + (t * each + k) * tail_rows
                final[t, k * own + head_rows : (k + 1) * own] = product[at : at + tail_rows]
    for d in reversed(range(1, nt)):
        away[d - 1][...] = final[peer_to(col, d, nt)].astype(bf16)
    mix[...] = final[col]
    for copies in y_copies + z_copies + [ez_copies, ey_copies]:
        for copy in copies:
            copy.wait_send()
    for pairs_of in gz_copies + gy_copies:
        for pair in pairs_of:
            for copy in pair:
                copy.wait_send()


def emit_kernel(
    states, next_in, next_write, next_read,
    states_h, next_in_h, next_write_h, next_read_h, sem,
):
    part = (DRAFT_TOKENS + 1) // 2
    pairs = [
        (states.at[s, pl.ds(t * part, part)], states_h.at[s, pl.ds(t * part, part)])
        for s in range(states.shape[0]) for t in range(2)
    ] + [
        (next_in, next_in_h), (next_write, next_write_h), (next_read, next_read_h),
    ]
    copies = [
        pltpu.make_async_copy(source, target, sem.at[i])
        for i, (source, target) in enumerate(pairs)
    ]
    for copy in copies:
        copy.start()
    for copy in copies:
        copy.wait()


def per_device(
    tokens, input_norm_gain, input_matrix, gate_matrix, write_matrix, read_matrix, step_matrix,
    input_kernel, write_kernel, read_kernel, step_size_bias, head_decay_logs, bypass_scale,
    extra_decay_logs, output_norm_gain, output_matrix, cached_state_history,
    cached_input_rows, cached_write_rows, cached_read_rows, accepted,
):
    kv = lax.axis_size("kv")
    nt = lax.axis_size("tp")
    nz, ny = factor(kv)
    own = tokens.shape[0] // kv
    head_rows = own - own % 16
    tail_rows = max(own - head_rows, 1)
    seqs = own // DRAFT_TOKENS
    full_rows = seqs * ROWS
    pad = -(-own // 16) * 16
    block = nz * own
    local = tokens.shape[1]
    heads = step_size_bias.shape[0]
    width = input_matrix.shape[1]
    sw = write_matrix.shape[1]
    group_width = width // (sw // N)
    groups = width // group_width
    half = group_width // 2
    out_width = output_matrix.shape[1]
    each = kv // nt
    vmem = pl.BlockSpec(memory_space=pltpu.VMEM)
    hbm = pl.BlockSpec(memory_space=pltpu.HBM)
    plan = [("write", 0, sw + 128), ("read", 0, sw)]
    plan += [("in", g * group_width, group_width) for g in reversed(range(groups))]
    plan += [("gate", g * group_width, group_width) for g in reversed(range(1, groups - 1))]
    if groups > 1:
        plan += [("gate", 0, half), ("gate", half, half)]
    sizes = [size for _, _, size in plan]
    pieces = len(plan)
    dma = pltpu.SemaphoreType.DMA
    peers = max(ny - 1, 1)
    shape = jax.ShapeDtypeStruct
    operands = (
        tokens, input_norm_gain[None], input_matrix, gate_matrix, write_matrix, read_matrix,
        step_matrix.T, step_size_bias[None], head_decay_logs[None], extra_decay_logs.T,
        input_kernel, write_kernel, read_kernel, bypass_scale[None], output_norm_gain[None],
        output_matrix, cached_state_history, cached_input_rows, cached_write_rows,
        cached_read_rows, accepted,
    )
    step_shape = (step_matrix.shape[1], local)
    buffers = [
        pltpu.VMEM(step_shape if i == 6 else a.shape, a.dtype)
        for i, a in enumerate(operands[:-1])
    ]
    part = (each * own, out_width)
    results = (
        (cached_state_history.shape, f32), (cached_input_rows.shape, bf16),
        (cached_write_rows.shape, bf16), (cached_read_rows.shape, bf16),
    )
    everything = ((part, f32),) + ((part, bf16),) * (nt - 1) + results
    outs = pl.pallas_call(
        functools.partial(
            mixer_kernel, nz, ny, nt, own, local * kv, tuple(plan), group_width
        ),
        out_shape=tuple(pltpu.VMEM(dims, kind) for dims, kind in everything),
        in_specs=[hbm] * len(operands),
        out_specs=[vmem] * len(everything),
        scratch_shapes=buffers + [
            pltpu.SMEM(accepted.shape, jnp.int32),
            dma((len(operands) + seqs,)),
            pltpu.VMEM(tokens.shape, f32),
            pltpu.VMEM((ny, block, local), f32),
            pltpu.VMEM((ny, block, local), bf16),
            pltpu.VMEM((ny, block, 128), f32),
            pltpu.VMEM((block, sum(sizes)), f32),
            pltpu.VMEM((block, max(sizes)), f32),
            pltpu.VMEM((pad, max(sizes)), f32),
            pltpu.VMEM((pad, width), f32),
            pltpu.VMEM((full_rows, heads), f32),
            pltpu.VMEM((full_rows, width), f32),
            pltpu.VMEM((full_rows, width), f32),
            pltpu.VMEM((full_rows, sw), f32),
            pltpu.VMEM((groups, kv, head_rows, group_width), bf16),
            pltpu.VMEM((groups, kv, tail_rows, group_width), bf16),
            pltpu.VMEM((groups, kv * tail_rows, group_width), f32),
            pltpu.VMEM((nt, each * own, out_width), f32),
            dma((pieces, peers)), dma((pieces, peers)),
            dma((pieces, nz - 1, 2)), dma((pieces, nz - 1, 2)),
            dma((groups, nz - 1, 2)), dma((groups, nz - 1, 2)),
            dma((groups, nz, peers, 2)), dma((groups, nz, peers, 2)),
            pltpu.VMEM((nz, ny, head_rows, group_width), bf16),
            pltpu.VMEM((nz, ny, tail_rows, group_width), bf16),
            pltpu.VMEM((nz - 1, ny, head_rows, group_width), bf16),
            pltpu.VMEM((nz - 1, ny, tail_rows, group_width), bf16),
            pltpu.VMEM((peers, head_rows, group_width), bf16),
            pltpu.VMEM((peers, tail_rows, group_width), bf16),
            pltpu.VMEM((peers, head_rows, group_width), bf16),
            pltpu.VMEM((peers, tail_rows, group_width), bf16),
            dma((nz - 1, 2)), dma((nz - 1, 2)), dma((peers, 2)), dma((peers, 2)),
        ]
        + [pltpu.VMEM((peers, block, c), bf16) for c in sizes]
        + [pltpu.VMEM((peers, block, c), bf16) for c in sizes]
        + [pltpu.VMEM((nz, head_rows, c), bf16) for c in sizes]
        + [pltpu.VMEM((nz, tail_rows, c), bf16) for c in sizes]
        + [pltpu.VMEM((nz - 1, head_rows, c), bf16) for c in sizes]
        + [pltpu.VMEM((nz - 1, tail_rows, c), bf16) for c in sizes],
        compiler_params=pltpu.CompilerParams(
            collective_id=0, has_side_effects=True, vmem_limit_bytes=40 * 2**20
        ),
    )(*[pltpu.with_memory_space_constraint(a, pltpu.HBM) for a in operands])
    kept = pl.pallas_call(
        emit_kernel,
        out_shape=tuple(shape(dims, kind) for dims, kind in results),
        in_specs=[vmem] * len(results),
        out_specs=[hbm] * len(results),
        scratch_shapes=[dma((seqs * 2 + len(results) - 1,))],
        compiler_params=pltpu.CompilerParams(vmem_limit_bytes=2**20),
        cost_estimate=pl.CostEstimate(flops=10**8, bytes_accessed=10**7, transcendentals=0),
    )(*outs[nt:])
    total = outs[0]
    for d in range(1, nt):
        ring = [(i, static_to(i, d, nt)) for i in range(nt)]
        total = total + lax.ppermute(outs[d], "tp", ring).astype(f32)
    return (total.astype(bf16),) + tuple(kept)


def solution(mesh):
    return jax.shard_map(
        per_device,
        mesh=mesh,
        in_specs=(
            P(None, "kv"),
            P("kv"),
            P("kv", "tp"),
            P("kv", "tp"),
            P("kv", "tp"),
            P("kv", "tp"),
            P(),
            P(None, "tp"),
            P(None, "tp"),
            P(None, "tp"),
            P("tp"),
            P("tp"),
            P("tp"),
            P("kv", "tp"),
            P("tp"),
            P("tp", "kv"),
            P("kv", None, "tp", None, None),
            P("kv", None, "tp"),
            P("kv", None, "tp"),
            P("kv", None, "tp"),
            P("kv"),
        ),
        out_specs=(
            P("tp", "kv"),
            P("kv", None, "tp", None, None),
            P("kv", None, "tp"),
            P("kv", None, "tp"),
            P("kv", None, "tp"),
        ),
        check_vma=False,
    )
```
